32 devices in a mesh: sp: 8 (over z, y), tp: 4 (over x, core).
Axes of the slice: x: 2, y: 2, z: 4, core: 2. Of those that a mesh axis runs over, the one named last changes fastest.
Arguments:
- resid_in: bfloat16 [3072, 2048], P('sp'), may hold values from -6 to 6
- cotangent: bfloat16 [3072, 2048], P('sp'), may hold values from -2 to 2
- norm_gain: float32 [2048], replicated, may hold values from 0.1 to 1.9
- routes: int32 [3072, 2], P('sp'), may hold values from 0 to 7, all different within a row; in each aligned block of 384 rows (0 to 383, 384 to 767, ...) at most 192 rows name the same one
- route_weights: float32 [3072, 2], P('sp'), may hold values from 0.1 to 1
- gate_weight: bfloat16 [8, 2048, 1024], P('sp', None, 'tp'), may hold values from -0.125 to 0.125
- up_weight: bfloat16 [8, 2048, 1024], P('sp', None, 'tp'), may hold values from -0.125 to 0.125
- down_weight: bfloat16 [8, 1024, 2048], P('sp', 'tp'), may hold values from -0.1875 to 0.1875
- out_weight: bfloat16 [2048, 1024], P(None, 'tp'), may hold values from -0.1875 to 0.1875
- gate_b: bfloat16 [3072, 1024], P('sp', 'tp'), may hold values from -6 to 6
- gate_c: bfloat16 [3072, 1024], P('sp', 'tp'), may hold values from -6 to 6
- values_u: bfloat16 [3072, 1024], P('sp', 'tp'), may hold values from -6 to 6
- taps: float32 [3, 1024], P(None, 'tp'), may hold values from -3.5 to 3.5
Outputs:
- grad_gate_weight: float32 [8, 2048, 1024], P('sp', None, 'tp')
- grad_up_weight: float32 [8, 2048, 1024], P('sp', None, 'tp')
- grad_down_weight: float32 [8, 1024, 2048], P('sp', 'tp')
- grad_resid: bfloat16 [3072, 2048], P('sp')
- grad_out_weight: float32 [2048, 1024], P('sp', 'tp')
- grad_gate_b: bfloat16 [3072, 1024], P('sp', 'tp')
- grad_gate_c: bfloat16 [3072, 1024], P('sp', 'tp')
- grad_values: bfloat16 [3072, 1024], P('sp', 'tp')
The draws below stay inside these ranges and needn't reach their ends.
Inputs may be any that keep to these rules, and one draw needn't show every extreme that they name: `routes`: A row's 2 experts differ. In the rows of one index of sp (384 tokens) no expert is named more than 192 times, a bound that some block reaches.
All inputs are finite; a program needn't handle non-finite values.
Results may differ from the reference program's by a relative error of at most 0.024.
Values may be sent and summed in bfloat16 or wider, within the bound.
A program may use at most 128 MiB of HBM per device.

```python
import math
import jax
import jax.numpy as jnp
import numpy as np
from jax import lax

D = 2048
SC = 1024
FF = 1024
TAPS = 3
TOP = 2
TOK_DEV = 384
EXPERTS = 8
CAP = 192
TOKENS = 3072
N_SP = 8
N_TP = 4


def with_spikes(entries, own_key, source, target, parts, factor):
    owner, partner = [(jnp.arange(entries.shape[axis_at]) // (entries.shape[axis_at] // parts)).reshape([-1 if axis == axis_at else 1 for axis in range(entries.ndim)]) for axis_at in (source, target)]
    chosen = jax.random.permutation(own_key, parts)[partner]
    strong = (owner == chosen) | (owner == (partner + parts // 2) % parts)
    return jnp.where(strong, factor * entries, entries)


def steps_of(key, shape, split, smallest, largest):
    factor_of, own = 1.0, jax.random.fold_in(key, 6)
    for position, blocks in split:
        draws = jnp.exp(jax.random.uniform(jax.random.fold_in(own, position), (blocks,), jnp.float32, smallest / len(split), largest / len(split)))
        factor_of = factor_of * jnp.repeat(draws, shape[position] // blocks).reshape([-1 if axis == position else 1 for axis in range(len(shape))])
    return factor_of


def deal_out(rng, own, number, rows, number_of, top, most, skew):
    sequence = jax.random.permutation(rng, number_of)
    heavy_load, common = shares(number_of, rows * top, most, skew, True), shares(number_of, rows * top, most, skew, False)
    places = jnp.arange(number_of)

    def named(tallies, rotation):
        used = int((tallies > 0).sum())
        fixed = max(1, used // 4)
        passed = fixed + (places - fixed + rotation * (used - fixed)) % max(1, number_of - fixed)
        return jnp.zeros((number_of,), jnp.int32).at[sequence[jnp.where(places < fixed, places, passed)]].set(jnp.asarray(tallies, jnp.int32))

    tallies = jnp.where(number % 4 == 0, named(heavy_load, number // 4), named(common, number - number // 4 - 1))
    mixed = jax.random.permutation(jax.random.fold_in(own, 3), number_of)
    source_of, receiver = mixed[0:number_of // 2 * 2:2], mixed[1:number_of // 2 * 2:2]
    room = jnp.minimum(tallies[source_of] - 1, most - tallies[receiver]) // 2
    room = jnp.where((source_of == sequence[0]) | (receiver == sequence[0]) | (tallies[receiver] == 0), 0, jnp.maximum(room, 0))
    passed = jax.random.randint(jax.random.fold_in(own, 4), (number_of // 2,), 0, 1 << 20) % (room + 1)
    tallies = tallies.at[source_of].add(-passed).at[receiver].add(passed)
    items = jnp.searchsorted(jnp.cumsum(tallies), jnp.arange(rows * top), side="right").astype(jnp.int32)
    listing = items.reshape(top, rows).T
    listing = listing[jax.random.permutation(jax.random.fold_in(own, 1), rows)]
    rotation = jax.random.randint(jax.random.fold_in(own, 2), (rows, 1), 0, top)
    return jnp.take_along_axis(listing, (jnp.arange(top)[None, :] + rotation) % top, axis=1)


def shares(number_of, total, reach, slope, full):
    portions = [(1 << 20) // math.isqrt(grade ** slope) + 1 for grade in range(1, number_of + 1)]
    largest = reach if full else min(reach, max(-(-total // number_of), total * portions[0] // sum(portions)))
    least = 1 if total - largest >= number_of - 1 else 0
    given, surplus = [largest] + [least] * (number_of - 1), total - largest - least * (number_of - 1)
    while surplus > 0:
        free = [i for i in range(1, number_of) if given[i] < largest] or [i for i in range(1, number_of) if given[i] < reach]
        pool, remaining = sum([portions[i] for i in free]), surplus
        for i in free:
            more = min(reach - given[i], max(1, remaining * portions[i] // pool), surplus)
            given[i] = given[i] + more
            surplus = surplus - more
    return np.array(given)


def gaussian(stream_key, extent, scale, reach, cuts=(), held_as=jnp.bfloat16):
    result = jax.random.normal(stream_key, extent, jnp.float32) * scale
    if len(cuts) > 0:
        result = steps_of(stream_key, extent, cuts, -0.22, 0.18) * result
    return jnp.clip(result, min=-reach, max=reach).astype(held_as)


def bell_draw_with(key, dims, spread, reach, pieces, heavy, held_as=jnp.bfloat16):
    drawn = spread * jax.random.normal(key, dims, jnp.float32)
    if pieces:
        drawn = drawn * steps_of(key, dims, pieces, -0.22, 0.18)
    return jnp.clip(with_spikes(drawn, jax.random.fold_in(key, 3), *heavy), -reach, reach).astype(held_as)


def setup_inputs(seed: int = 0) -> dict:
    arg_keys = jax.random.split(jax.random.key(seed), 14)
    resid_in = gaussian(arg_keys[0], (TOKENS, D), 1.0, 6.0, ((0, 8),))
    cotangent = bell_draw_with(arg_keys[1], (TOKENS, D), 0.25, 2.0, ((0, 8),), (0, 1, 8, 2.0))
    norm_gain = jnp.clip(1.0 + 0.18 * jax.random.normal(arg_keys[2], (D,), jnp.float32), 0.1, 1.9)
    routes_keys = jax.random.split(jax.random.fold_in(arg_keys[3], 1), TOKENS // TOK_DEV)
    routes_turns = jax.random.permutation(jax.random.fold_in(arg_keys[3], 3), TOKENS // TOK_DEV)
    routes = jax.vmap(lambda own, number: deal_out(jax.random.fold_in(arg_keys[3], 2), own, number, TOK_DEV, EXPERTS, TOP, CAP, 1))(routes_keys, routes_turns).reshape((TOKENS, TOP))
    route_weights = jnp.clip(0.1 + 0.9 * jax.random.uniform(arg_keys[4], (TOKENS, TOP), jnp.float32) ** steps_of(arg_keys[4], (TOKENS, TOP), ((0, 8),), -0.2, 0.2), 0.1, 1.0)
    gate_weight = gaussian(arg_keys[5], (EXPERTS, D, FF), D ** -0.5, 0.125, ((0, 8), (2, 4)))
    up_weight = gaussian(arg_keys[6], (EXPERTS, D, FF), D ** -0.5, 0.125, ((0, 8), (2, 4)))
    down_weight = gaussian(arg_keys[7], (EXPERTS, FF, D), FF ** -0.5, 0.1875, ((0, 8), (1, 4)))
    out_weight = gaussian(arg_keys[8], (D, SC), SC ** -0.5, 0.1875, ((1, 4),))
    gate_b = gaussian(arg_keys[9], (TOKENS, SC), 1.0, 6.0, ((0, 8), (1, 4)))
    gate_c = gaussian(arg_keys[10], (TOKENS, SC), 1.0, 6.0, ((0, 8), (1, 4)))
    values_u = gaussian(arg_keys[11], (TOKENS, SC), 1.0, 6.0, ((0, 8), (1, 4)))
    taps = gaussian(arg_keys[12], (TAPS, SC), TAPS ** -0.5, 3.5, ((1, 4),), jnp.float32)
    return dict(resid_in=resid_in, cotangent=cotangent, norm_gain=norm_gain, routes=routes, route_weights=route_weights, gate_weight=gate_weight, up_weight=up_weight, down_weight=down_weight, out_weight=out_weight, gate_b=gate_b, gate_c=gate_c, values_u=values_u, taps=taps)


norm_eps = 1e-06

def expert_pass(entry_rows, entry_cots, entry_weights, gate_mat, up_mat, down_mat):
    f32 = jnp.float32
    bf16 = jnp.bfloat16
    gate_pre = jnp.dot(entry_rows, gate_mat, preferred_element_type=f32)
    up_pre = jnp.dot(entry_rows, up_mat, preferred_element_type=f32)
    logistic = jax.nn.sigmoid(gate_pre)
    activated = gate_pre * logistic
    hidden = (activated * up_pre * entry_weights[:, None]).astype(bf16)
    grad_down = jnp.dot(hidden.T, entry_cots, preferred_element_type=f32)
    dhidden = jnp.dot(entry_cots, down_mat.T, preferred_element_type=f32) * entry_weights[:, None]
    dgate = (dhidden * up_pre * logistic * (1.0 + gate_pre * (1.0 - logistic))).astype(bf16)
    dup = (dhidden * activated).astype(bf16)
    grad_gate = jnp.dot(entry_rows.T, dgate, preferred_element_type=f32)
    grad_up = jnp.dot(entry_rows.T, dup, preferred_element_type=f32)
    quarter = gate_mat.shape[1] // N_TP
    summed = jnp.zeros((entry_rows.shape[0], entry_rows.shape[1]), f32)
    for lane_index in range(N_TP):
        lower = lane_index * quarter
        upper = lower + quarter
        partial_sum = jnp.dot(dgate[:, lower:upper], gate_mat[:, lower:upper].T, preferred_element_type=f32) + jnp.dot(dup[:, lower:upper], up_mat[:, lower:upper].T, preferred_element_type=f32)
        summed = summed + lax.optimization_barrier(partial_sum.astype(bf16)).astype(f32)
    return (grad_gate, grad_up, grad_down, summed.astype(bf16))

def reference(resid_in, cotangent, norm_gain, routes, route_weights, gate_weight, up_weight, down_weight, out_weight, gate_b, gate_c, values_u, taps):
    f32 = jnp.float32
    bf16 = jnp.bfloat16
    token_total = resid_in.shape[0]
    resid_wide = resid_in.astype(f32)
    inv_rms = lax.rsqrt(lax.optimization_barrier(jnp.mean(resid_wide * resid_wide, axis=1, keepdims=True)) + norm_eps)
    normed = (resid_wide * inv_rms * norm_gain).astype(bf16)
    flat_routes = routes.reshape(-1).astype(jnp.int32)
    flat_weights = route_weights.reshape(-1)
    slot_total = N_SP * CAP

    def one_expert(expert_id):
        chosen = flat_routes == expert_id
        found = jnp.nonzero(chosen, size=slot_total, fill_value=0)[0].astype(jnp.int32)
        how_many = jnp.sum(chosen.astype(jnp.int32))
        is_valid = jnp.arange(slot_total, dtype=jnp.int32) < how_many
        owners = found // 2
        entry_weights = jnp.where(is_valid, flat_weights[found], jnp.zeros((), f32))
        grads = expert_pass(normed[owners], cotangent[owners], entry_weights, gate_weight[expert_id], up_weight[expert_id], down_weight[expert_id])
        targets = jnp.where(is_valid, found, 2 * token_total).astype(jnp.int32)
        return (grads[0], grads[1], grads[2], grads[3], targets)
    grad_gate_weight, grad_up_weight, grad_down_weight, slot_rows, targets = lax.map(one_expert, jnp.arange(EXPERTS, dtype=jnp.int32))
    slot_grads = jnp.zeros((2 * token_total + 1, D), f32).at[targets.reshape(-1)].add(slot_rows.reshape(-1, D).astype(f32))
    paired = slot_grads[:2 * token_total].reshape(token_total, 2, D)
    dnormed = paired[:, 0] + paired[:, 1]
    scaled = dnormed * norm_gain
    resid_grad = cotangent.astype(f32) + inv_rms * scaled - resid_wide * inv_rms ** 3 * lax.optimization_barrier(jnp.mean(scaled * resid_wide, axis=1, keepdims=True))
    grad_resid = resid_grad.astype(bf16)
    mixed = gate_c.astype(f32) * values_u.astype(f32)
    padded = jnp.pad(mixed, ((2, 0), (0, 0)))
    conv = taps[0] * padded[:-2] + taps[1] * padded[1:-1] + taps[2] * padded[2:]
    merged = (gate_b.astype(f32) * conv).astype(bf16)
    grad_out_weight = jnp.dot(grad_resid.T, merged, preferred_element_type=f32)
    dmerged = jnp.dot(grad_resid, out_weight, preferred_element_type=f32)
    grad_gate_b = (dmerged * conv).astype(bf16)
    dconv = dmerged * gate_b.astype(f32)
    padded_grad = jnp.pad(dconv, ((0, 2), (0, 0)))
    dmixed = taps[2] * padded_grad[:-2] + taps[1] * padded_grad[1:-1] + taps[0] * padded_grad[2:]
    grad_gate_c = (dmixed * values_u.astype(f32)).astype(bf16)
    grad_values = (dmixed * gate_c.astype(f32)).astype(bf16)
    return (grad_gate_weight, grad_up_weight, grad_down_weight, grad_resid, grad_out_weight, grad_gate_b, grad_gate_c, grad_values)
```

```python
import functools

import jax
import jax.numpy as jnp
from jax import lax
from jax.experimental import pallas as pl
from jax.experimental.pallas import tpu as pltpu
from jax.sharding import PartitionSpec as P

norm_eps = 1e-06


def passed_along(array, axis, by):
    size = lax.axis_size(axis)
    pairs = [(i, i + by) for i in range(size) if 0 <= i + by < size]
    return lax.ppermute(array, axis, pairs)


def remote(source, target, send_sem, recv_sem, **device):
    return pltpu.make_async_remote_copy(
        src_ref=source,
        dst_ref=target,
        send_sem=send_sem,
        recv_sem=recv_sem,
        device_id=device,
        device_id_type=pl.DeviceIdType.MESH,
    )


def greet(groups, spot, core_peer, far_peer):
    barrier = pltpu.get_barrier_semaphore()

    def to_group(offset, carry):
        pl.semaphore_signal(
            barrier,
            inc=1,
            device_id={"sp": lax.rem(spot + offset, groups)},
            device_id_type=pl.DeviceIdType.MESH,
        )
        return carry

    lax.fori_loop(1, groups, to_group, 0)
    for peer in (core_peer, far_peer):
        pl.semaphore_signal(
            barrier, inc=1, device_id={"tp": peer}, device_id_type=pl.DeviceIdType.MESH
        )
    pl.semaphore_wait(barrier, groups + 1)


def expert_kernel(
    groups,
    width,
    lanes,
    normed,
    cots,
    info,
    gate_mat,
    up_mat,
    down_mat,
    returned,
    gate_out,
    up_out,
    down_out,
    infos,
    dense,
    to_mate,
    to_mate_own,
    rows,
    row_cots,
    hidden,
    dgate,
    dup,
    partial,
    from_core,
    to_far,
    from_far,
    summed,
    grad_a,
    grad_b,
    local_sem,
    send_i,
    recv_i,
    send_z,
    recv_z,
    send_y,
    recv_y,
    send_o,
    recv_o,
    send_x,
    recv_x,
    send_c,
    recv_c,
    send_f,
    recv_f,
    send_t,
    recv_t,
    send_r,
    recv_r,
    send_h,
    recv_h,
):
    f32 = jnp.float32
    bf16 = jnp.bfloat16
    spot, lane = lax.axis_index("sp"), lax.axis_index("tp")
    depth = groups // width
    z, y = lax.div(spot, width), lax.rem(spot, width)
    core = lax.rem(lane, 2)
    core_peer = lane + 1 - 2 * core
    far_peer = lax.rem(lane + lanes // 2, lanes)
    mate = spot + 1 - 2 * y
    token_count, model_width = normed.shape
    quarter = model_width // lanes
    half = model_width // 2
    span = rows.shape[1]
    given = (normed, cots)
    laid = (rows, row_cots)

    def columns(who, size):
        return pl.ds(pl.multiple_of(who * size, size), size)

    def part(ref, block, who):
        return ref.at[block, :, columns(who, quarter)]

    def source(side, level):
        return z + level * (2 * side - 1)

    def valid(side, level):
        at = source(side, level)
        there = jnp.logical_and(at >= 0, at < depth)
        return jnp.logical_and(there, jnp.logical_or(level > 0, side == 0))

    def onward(side):
        at = z + 1 - 2 * side
        return jnp.logical_and(at >= 0, at < depth)

    def block_of(side, level, line):
        return source(side, level) * width + lax.rem(y + line, width)

    def tell(offset):
        goal = lax.rem(spot + offset, groups)
        return remote(info, infos.at[spot], send_i.at[offset], recv_i.at[spot], sp=goal)

    def told(offset):
        origin = lax.rem(spot - offset + groups, groups)
        return remote(info, infos.at[origin], send_i.at[offset], recv_i.at[origin], sp=origin)

    def hop(k, at, side, own):
        held = dense.at[k, at]
        return remote(
            given[k].at[:, columns(lane, quarter)] if own else held,
            held,
            send_z.at[k, side, at],
            recv_z.at[k, at],
            sp=spot + width * (1 - 2 * side),
        )

    def over(k, at):
        return remote(
            to_mate.at[k, at],
            part(laid[k], at * width + y, lane),
            send_y.at[k, at],
            recv_y.at[k, at],
            sp=mate,
        )

    def over_own(k):
        return remote(
            to_mate_own.at[k],
            laid[k].at[spot, :, columns(core, half)],
            send_o.at[k],
            recv_o.at[k],
            sp=mate,
        )

    def far_copy(k, block):
        held = part(laid[k], block, lane)
        return remote(held, held, send_x.at[k, block], recv_x.at[k, block], tp=far_peer)

    def core_copy(k, block):
        held = part(laid[k], block, lane)
        return remote(held, held, send_c.at[k, block], recv_c.at[k, block], tp=core_peer)

    def half_copy(k):
        held = laid[k].at[mate, :, columns(core, half)]
        return remote(held, held, send_c.at[k, mate], recv_c.at[k, mate], tp=core_peer)

    def pass_copy(k, block):
        held = part(laid[k], block, far_peer)
        return remote(held, held, send_f.at[k, block], recv_f.at[k, block], tp=core_peer)

    def to_core(block, far):
        who = lax.rem(core_peer + far * (lanes // 2), lanes)
        return remote(
            part(partial, block, who),
            from_core.at[block, far],
            send_t.at[block, far],
            recv_t.at[block, far],
            tp=core_peer,
        )

    def to_far_peer(block):
        return remote(
            to_far.at[block],
            from_far.at[block],
            send_r.at[block],
            recv_r.at[block],
            tp=far_peer,
        )

    def home(block):
        return remote(
            summed.at[block], returned.at[spot], send_h.at[block], recv_h.at[spot], sp=block
        )

    def home_from(block):
        return remote(
            summed.at[block], returned.at[block], send_h.at[block], recv_h.at[block], sp=block
        )

    def matches(block, expert):
        slot = lax.broadcasted_iota(jnp.int32, (span, token_count), 0) + expert * span
        slot = slot.astype(f32)
        return slot == infos[block, 0:1, :], slot == infos[block, 1:2, :]

    def chosen(block, expert):
        first, second = matches(block, expert)
        return jnp.where(jnp.logical_or(first, second), 1.0, 0.0).astype(bf16)

    def weights_of(block):
        first, second = matches(block, spot)
        return jnp.sum(
            jnp.where(first, infos[block, 2:3, :], 0.0)
            + jnp.where(second, infos[block, 3:4, :], 0.0),
            axis=1,
            keepdims=True,
        )

    def placed(matrix, values):
        return jnp.dot(matrix, values, preferred_element_type=f32).astype(bf16)

    def both(body):
        def step(side, carry):
            body(side)
            return carry

        lax.fori_loop(0, 2, step, 0)

    def each_block(level, body):
        def step(at, carry):
            side, line = lax.div(at, 2), lax.rem(at, 2)

            @pl.when(valid(side, level))
            def _():
                body(block_of(side, level, line), side, line)

            return carry

        lax.fori_loop(0, 4, step, 0)

    core_side, far_side = core_peer, far_peer
    greet(groups, spot, core_side, far_side)

    def tell_all(offset, carry):
        tell(offset).start()
        return carry

    lax.fori_loop(1, groups, tell_all, 0)
    for k in (0, 1):
        for side in (0, 1):

            @pl.when(onward(side))
            def _():
                hop(k, z, side, True).start()

    infos[spot] = info[...]
    mine_there = chosen(spot, mate)
    for k in (0, 1):
        to_mate_own[k] = placed(mine_there, given[k][:, columns(core, half)])
        over_own(k).start()
    mine_here = chosen(spot, spot)

    def lay_own(at, carry):
        for k in (0, 1):
            laid[k][spot, :, columns(at, quarter)] = placed(
                mine_here, given[k][:, columns(at, quarter)]
            )
        return carry

    lax.fori_loop(0, lanes, lay_own, 0)

    def hear_all(offset, carry):
        told(offset).wait_recv()
        return carry

    lax.fori_loop(1, groups, hear_all, 0)

    def dispatch_level(level):
        for k in (0, 1):

            def take(side):
                @pl.when(valid(side, level))
                def _():
                    at = source(side, level)
                    hop(k, at, side, False).wait_recv()

                    @pl.when(onward(side))
                    def _():
                        hop(k, at, side, False).start()

            both(take)

            def place(side):
                @pl.when(valid(side, level))
                def _():
                    at = source(side, level)
                    block = at * width + y
                    values = dense[k, at]
                    to_mate[k, at] = placed(chosen(block, mate), values)
                    over(k, at).start()
                    laid[k][block, :, columns(lane, quarter)] = placed(
                        chosen(block, spot), values
                    )
                    far_copy(k, block).start()
                    core_copy(k, block).start()

            both(place)

        def receive(side):
            @pl.when(valid(side, level))
            def _():
                at = source(side, level)
                block = at * width + 1 - y
                for k in (0, 1):
                    over(k, at).wait_recv()
                    far_copy(k, block).start()
                    core_copy(k, block).start()

        both(receive)

    def share_level(level):
        @pl.when(level == 0)
        def _():
            for k in (0, 1):
                over_own(k).wait_recv()
                half_copy(k).start()

        def share(block, side, line):
            @pl.when(level > 0)
            def _():
                for k in (0, 1):
                    far_copy(k, block).wait_recv()
                    pass_copy(k, block).start()

        each_block(level, share)

    def compute_level(level):
        def compute(block, side, line):
            @pl.when(level > 0)
            def _():
                for k in (0, 1):
                    core_copy(k, block).wait_recv()
                    pass_copy(k, block).wait_recv()

            @pl.when(jnp.logical_and(level == 0, line == 1))
            def _():
                for k in (0, 1):
                    half_copy(k).wait_recv()

            weight = weights_of(block)
            entry_rows = rows[block]
            gate_pre = jnp.dot(entry_rows, gate_mat[...], preferred_element_type=f32)
            up_pre = jnp.dot(entry_rows, up_mat[...], preferred_element_type=f32)
            pulled = lax.dot_general(
                row_cots[block],
                down_mat[...],
                (((1,), (1,)), ((), ())),
                preferred_element_type=f32,
            )
            logistic = jax.nn.sigmoid(gate_pre)
            activated = gate_pre * logistic
            hidden[block] = (activated * up_pre * weight).astype(bf16)
            dhidden = pulled * weight
            grad_gate = (
                dhidden * up_pre * logistic * (1.0 + gate_pre * (1.0 - logistic))
            ).astype(bf16)
            grad_up = (dhidden * activated).astype(bf16)
            dgate[block] = grad_gate
            dup[block] = grad_up

            def back(at, carry):
                picked = columns(at, quarter)
                over_width = (((1,), (1,)), ((), ()))
                partial[block, :, picked] = (
                    lax.dot_general(
                        grad_gate, gate_mat[picked, :], over_width, preferred_element_type=f32
                    )
                    + lax.dot_general(
                        grad_up, up_mat[picked, :], over_width, preferred_element_type=f32
                    )
                ).astype(bf16)
                return carry

            lax.fori_loop(0, lanes, back, 0)
            to_core(block, 1).start()
            to_core(block, 0).start()

        each_block(level, compute)

    def middle_level(level):
        def middle(block, side, line):
            to_core(block, 1).wait_recv()
            to_far[block] = (
                partial[block, :, columns(far_peer, quarter)].astype(f32)
                + from_core[block, 1].astype(f32)
            ).astype(bf16)
            to_far_peer(block).start()

        each_block(level, middle)

    def total_level(level):
        def total(block, side, line):
            to_core(block, 0).wait_recv()
            to_far_peer(block).wait_recv()
            value = (
                partial[block, :, columns(lane, quarter)].astype(f32)
                + from_core[block, 0].astype(f32)
                + from_far[block].astype(f32)
            ).astype(bf16)

            @pl.when(block == spot)
            def _():
                returned[spot] = value

            @pl.when(block != spot)
            def _():
                summed[block] = value
                home(block).start()

        each_block(level, total)

    def weight_grads():
        slots = groups * span
        down_in = (((0,), (0,)), ((), ()))

        def down_step(at, carry):
            picked = columns(at, quarter)
            grad_b[:, picked] = lax.dot_general(
                hidden[...].reshape(slots, hidden.shape[2]),
                row_cots[:, :, picked].reshape(slots, quarter),
                down_in,
                preferred_element_type=f32,
            )
            return carry

        lax.fori_loop(0, lanes, down_step, 0)
        down_copy = pltpu.make_async_copy(grad_b, down_out, local_sem.at[0])
        down_copy.start()
        copies = [down_copy]
        for spread, out, index in ((dgate, gate_out, 0), (dup, up_out, 1)):

            def step(at, carry):
                picked = columns(at, quarter)
                grad_a[index, picked, :] = lax.dot_general(
                    rows[:, :, picked].reshape(slots, quarter),
                    spread[...].reshape(slots, spread.shape[2]),
                    down_in,
                    preferred_element_type=f32,
                )
                return carry

            lax.fori_loop(0, lanes, step, 0)
            copy = pltpu.make_async_copy(grad_a.at[index], out, local_sem.at[index + 1])
            copy.start()
            copies.append(copy)
        for copy in copies:
            copy.wait()

    def advance(level, carry):
        dispatch_level(level)
        share_level(level - 1)
        compute_level(level - 1)

        @pl.when(level >= 2)
        def _():
            middle_level(level - 2)

        @pl.when(level >= 3)
        def _():
            total_level(level - 3)

        return carry

    lax.fori_loop(1, depth + 1, advance, 0)
    middle_level(depth - 1)
    total_level(depth - 2)
    weight_grads()
    total_level(depth - 1)

    def finish_info(offset, carry):
        tell(offset).wait_send()
        origin = lax.rem(spot + offset, groups)
        home_from(origin).wait()
        return carry

    lax.fori_loop(1, groups, finish_info, 0)
    for k in (0, 1):
        for side in (0, 1):

            @pl.when(onward(side))
            def _():
                hop(k, z, side, True).wait_send()

        over_own(k).wait_send()
        half_copy(k).wait_send()

    def finish_level(level, carry):
        def finish(block, side, line):
            to_core(block, 0).wait_send()
            to_core(block, 1).wait_send()
            to_far_peer(block).wait_send()

            @pl.when(level > 0)
            def _():
                for k in (0, 1):
                    far_copy(k, block).wait_send()
                    core_copy(k, block).wait_send()
                    pass_copy(k, block).wait_send()

            @pl.when(jnp.logical_and(level > 0, line == 0))
            def _():
                at = source(side, level)
                for k in (0, 1):
                    over(k, at).wait_send()

                    @pl.when(onward(side))
                    def _():
                        hop(k, at, side, False).wait_send()

        each_block(level, finish)
        return carry

    lax.fori_loop(0, depth, finish_level, 0)


def experts(normed, cots, info, gate_mat, up_mat, down_mat, groups, lanes, span):
    token_count, model_width = normed.shape
    inner = gate_mat.shape[1]
    quarter = model_width // lanes
    width = 2
    depth = groups // width
    bf16, f32 = jnp.bfloat16, jnp.float32
    dma = pltpu.SemaphoreType.DMA
    inside = pl.BlockSpec(memory_space=pltpu.VMEM)
    anywhere = pl.BlockSpec(memory_space=pl.ANY)
    block = (groups, span, quarter)
    whole = (groups, span, model_width)
    thin = (groups, span, inner)
    vmem = pltpu.VMEM
    return pl.pallas_call(
        functools.partial(expert_kernel, groups, width, lanes),
        out_shape=(
            jax.ShapeDtypeStruct(block, bf16),
            jax.ShapeDtypeStruct(gate_mat.shape, f32),
            jax.ShapeDtypeStruct(up_mat.shape, f32),
            jax.ShapeDtypeStruct(down_mat.shape, f32),
        ),
        in_specs=[inside] * 6,
        out_specs=(inside, anywhere, anywhere, anywhere),
        scratch_shapes=[
            vmem((groups,) + info.shape, f32),
            vmem((2, depth, token_count, quarter), bf16),
            vmem((2, depth, span, quarter), bf16),
            vmem((2, span, model_width // 2), bf16),
            vmem(whole, bf16),
            vmem(whole, bf16),
            vmem(thin, bf16),
            vmem(thin, bf16),
            vmem(thin, bf16),
            vmem(whole, bf16),
            vmem((groups, 2, span, quarter), bf16),
            vmem(block, bf16),
            vmem(block, bf16),
            vmem(block, bf16),
            vmem((2,) + gate_mat.shape, f32),
            vmem(down_mat.shape, f32),
            dma((3,)),
            dma((groups,)),
            dma((groups,)),
            dma((2, 2, depth)),
            dma((2, depth)),
            dma((2, depth)),
            dma((2, depth)),
            dma((2,)),
            dma((2,)),
        ]
        + [dma((2, groups))] * 6
        + [dma((groups, 2))] * 2
        + [dma((groups,))] * 4,
        compiler_params=pltpu.CompilerParams(
            collective_id=1, has_side_effects=True, vmem_limit_bytes=63 * 2**20
        ),
        cost_estimate=pl.CostEstimate(
            flops=16 * groups * span * model_width * inner,
            bytes_accessed=150 * 2**20,
            transcendentals=0,
        ),
        name="experts",
    )(normed, cots, info, gate_mat, up_mat, down_mat)


def gather_kernel(groups, lanes, mine, gathered, own_sem, send_sems, recv_sems):
    spot, lane = lax.axis_index("sp"), lax.axis_index("tp")
    core_peer = lane + 1 - 2 * lax.rem(lane, 2)
    far_peer = lax.rem(lane + lanes // 2, lanes)
    quarter = mine.shape[1]

    def part(who):
        return gathered.at[:, pl.ds(pl.multiple_of(who * quarter, quarter), quarter)]

    greet(groups, spot, core_peer, far_peer)
    far = remote(mine, part(lane), send_sems.at[0], recv_sems.at[0], tp=far_peer)
    near = remote(mine, part(lane), send_sems.at[1], recv_sems.at[1], tp=core_peer)
    own = pltpu.make_async_copy(mine, part(lane), own_sem)
    far.start()
    near.start()
    own.start()
    far.wait_recv()
    passed = remote(
        part(far_peer), part(far_peer), send_sems.at[2], recv_sems.at[2], tp=core_peer
    )
    passed.start()
    far.wait_send()
    near.wait()
    own.wait()
    passed.wait()


def gather_quarters(mine, groups, lanes):
    sem = pltpu.SemaphoreType.DMA
    inside = pl.BlockSpec(memory_space=pltpu.VMEM)
    return pl.pallas_call(
        functools.partial(gather_kernel, groups, lanes),
        out_shape=jax.ShapeDtypeStruct((mine.shape[0], mine.shape[1] * lanes), mine.dtype),
        in_specs=[inside],
        out_specs=inside,
        scratch_shapes=[sem, sem((3,)), sem((3,))],
        compiler_params=pltpu.CompilerParams(collective_id=3, has_side_effects=True),
        name="gather_quarters",
    )(mine)


def reduce_kernel(groups, lanes, partial, total, arrived, send_sems, recv_sems):
    f32 = jnp.float32
    spot, lane = lax.axis_index("sp"), lax.axis_index("tp")
    core_peer = lane + 1 - 2 * lax.rem(lane, 2)
    far_peer = lax.rem(lane + lanes // 2, lanes)

    def across(offset):
        goal = lax.rem(spot + offset, groups)
        return remote(
            partial.at[goal],
            arrived.at[offset],
            send_sems.at[offset],
            recv_sems.at[offset],
            sp=goal,
        )

    greet(groups, spot, core_peer, far_peer)

    def launch(offset, carry):
        across(offset).start()
        return carry

    lax.fori_loop(1, groups, launch, 0)
    total[...] = partial[spot].astype(f32)

    def add(offset, carry):
        across(offset).wait_recv()
        total[...] += arrived[offset].astype(f32)
        return carry

    lax.fori_loop(1, groups, add, 0)

    def finish(offset, carry):
        across(offset).wait_send()
        return carry

    lax.fori_loop(1, groups, finish, 0)


def reduce_rows(partial, groups, lanes):
    sem = pltpu.SemaphoreType.DMA
    inside = pl.BlockSpec(memory_space=pltpu.VMEM)
    return pl.pallas_call(
        functools.partial(reduce_kernel, groups, lanes),
        out_shape=jax.ShapeDtypeStruct(partial.shape[1:], jnp.float32),
        in_specs=[inside],
        out_specs=inside,
        scratch_shapes=[
            pltpu.VMEM(partial.shape, partial.dtype),
            sem((groups,)),
            sem((groups,)),
        ],
        compiler_params=pltpu.CompilerParams(collective_id=4, has_side_effects=True),
        name="reduce_rows",
    )(partial)


def on_device(
    resid_in,
    cotangent,
    norm_gain,
    routes,
    route_weights,
    gate_weight,
    up_weight,
    down_weight,
    out_weight,
    gate_b,
    gate_c,
    values_u,
    taps,
):
    f32 = jnp.float32
    bf16 = jnp.bfloat16
    token_count, model_width = resid_in.shape
    groups = lax.axis_size("sp")
    lanes = lax.axis_size("tp")
    local_experts = gate_weight.shape[0]
    expert_total = local_experts * groups
    capacity = 4 * token_count // expert_total
    slot_span = local_experts * capacity
    resid_wide = resid_in.astype(f32)
    inv_rms = lax.rsqrt(jnp.mean(resid_wide * resid_wide, axis=1, keepdims=True) + norm_eps)
    normed = (resid_wide * inv_rms * norm_gain).astype(bf16)
    mixed = gate_c.astype(f32) * values_u.astype(f32)
    earlier = passed_along(mixed[-2:], "sp", 1)
    quarter = model_width // lanes
    slots = expert_total * capacity
    names = jnp.arange(expert_total, dtype=jnp.int32)
    chosen = routes[:, :, None] == names[None, None, :]
    named = jnp.any(chosen, axis=1).astype(bf16)
    order = jnp.arange(token_count, dtype=jnp.int32)
    strict = (order[:, None] > order[None, :]).astype(bf16)
    before = jnp.dot(strict, named, preferred_element_type=f32).astype(jnp.int32)
    rank = jnp.sum(jnp.where(chosen, before[:, None, :], 0), axis=2)
    targets = routes * capacity + rank
    slot_ids = jnp.arange(slots, dtype=jnp.int32)[:, None]
    first = slot_ids == targets[:, 0][None, :]
    second = slot_ids == targets[:, 1][None, :]
    placing = (first | second).astype(bf16)
    info = jnp.concatenate(
        [
            targets.T.astype(f32),
            route_weights.T,
            jnp.zeros((4, token_count), f32),
        ],
        axis=0,
    )
    returned, grad_gate, grad_up, grad_down = experts(
        normed,
        cotangent,
        info,
        gate_weight[0],
        up_weight[0],
        down_weight[0],
        groups,
        lanes,
        slot_span,
    )
    returned = returned.reshape(slots, quarter)
    own_grad = jnp.einsum("st,sq->tq", placing, returned, preferred_element_type=f32)
    dnormed = gather_quarters(own_grad.astype(bf16), groups, lanes).astype(f32)
    scaled = dnormed * norm_gain
    resid_grad = (
        cotangent.astype(f32)
        + inv_rms * scaled
        - resid_wide * inv_rms**3 * jnp.mean(scaled * resid_wide, axis=1, keepdims=True)
    )
    grad_resid = resid_grad.astype(bf16)
    extended = jnp.concatenate([earlier, mixed], axis=0)
    conv = (
        taps[0] * extended[:token_count]
        + taps[1] * extended[1 : token_count + 1]
        + taps[2] * extended[2 : token_count + 2]
    )
    merged = (gate_b.astype(f32) * conv).astype(bf16)
    out_partial = jnp.einsum("td,tc->dc", grad_resid, merged, preferred_element_type=f32)
    grad_out_weight = reduce_rows(
        out_partial.astype(bf16).reshape(groups, model_width // groups, merged.shape[1]),
        groups,
        lanes,
    )
    dmerged = jnp.dot(grad_resid, out_weight, preferred_element_type=f32)
    grad_gate_b = (dmerged * conv).astype(bf16)
    dconv = dmerged * gate_b.astype(f32)
    later = passed_along(dconv[:2], "sp", -1)
    extended_grad = jnp.concatenate([dconv, later], axis=0)
    dmixed = (
        taps[2] * extended_grad[:token_count]
        + taps[1] * extended_grad[1 : token_count + 1]
        + taps[0] * extended_grad[2 : token_count + 2]
    )
    grad_gate_c = (dmixed * values_u.astype(f32)).astype(bf16)
    grad_values = (dmixed * gate_c.astype(f32)).astype(bf16)
    return (
        grad_gate[None],
        grad_up[None],
        grad_down[None],
        grad_resid,
        grad_out_weight,
        grad_gate_b,
        grad_gate_c,
        grad_values,
    )


def solution(mesh):
    placed = (
        P("sp", None),
        P("sp", None),
        P(),
        P("sp", None),
        P("sp", None),
        P("sp", None, "tp"),
        P("sp", None, "tp"),
        P("sp", "tp", None),
        P(None, "tp"),
        P("sp", "tp"),
        P("sp", "tp"),
        P("sp", "tp"),
        P(None, "tp"),
    )
    return jax.shard_map(
        on_device,
        mesh=mesh,
        in_specs=placed,
        out_specs=(
            P("sp", None, "tp"),
            P("sp", None, "tp"),
            P("sp", "tp", None),
            P("sp", None),
            P("sp", "tp"),
            P("sp", "tp"),
            P("sp", "tp"),
            P("sp", "tp"),
        ),
        check_vma=False,
    )
```

```python
import functools

import jax
import jax.numpy as jnp
from jax import lax
from jax.experimental import pallas as pl
from jax.experimental.pallas import tpu as pltpu
from jax.sharding import PartitionSpec as P

norm_eps = 1e-06


def passed_along(array, axis, by):
    size = lax.axis_size(axis)
    pairs = [(i, i + by) for i in range(size) if 0 <= i + by < size]
    return lax.ppermute(array, axis, pairs)


def remote(source, target, send_sem, recv_sem, **device):
    return pltpu.make_async_remote_copy(
        src_ref=source,
        dst_ref=target,
        send_sem=send_sem,
        recv_sem=recv_sem,
        device_id=device,
        device_id_type=pl.DeviceIdType.MESH,
    )


def greet(groups, spot, core_peer, far_peer):
    barrier = pltpu.get_barrier_semaphore()

    def to_group(offset, carry):
        pl.semaphore_signal(
            barrier,
            inc=1,
            device_id={"sp": lax.rem(spot + offset, groups)},
            device_id_type=pl.DeviceIdType.MESH,
        )
        return carry

    lax.fori_loop(1, groups, to_group, 0)
    for peer in (core_peer, far_peer):
        pl.semaphore_signal(
            barrier, inc=1, device_id={"tp": peer}, device_id_type=pl.DeviceIdType.MESH
        )
    pl.semaphore_wait(barrier, groups + 1)


def expert_kernel(
    groups,
    width,
    lanes,
    normed,
    cots,
    info,
    targets,
    gate_mat,
    up_mat,
    down_mat,
    gathered,
    gate_out,
    up_out,
    down_out,
    infos,
    dense,
    dense_wide,
    to_mate,
    to_mate_wide,
    to_mate_own,
    rows,
    row_cots,
    hidden,
    dgate,
    dup,
    partial,
    from_core,
    to_far,
    from_far,
    summed,
    returned,
    combined,
    grad_a,
    grad_b,
    local_sem,
    send_i,
    recv_i,
    send_z,
    recv_z,
    send_y,
    recv_y,
    send_o,
    recv_o,
    send_x,
    recv_x,
    send_c,
    recv_c,
    send_f,
    recv_f,
    send_t,
    recv_t,
    send_r,
    recv_r,
    send_h,
    recv_h,
    send_g,
    recv_g,
):
    f32 = jnp.float32
    bf16 = jnp.bfloat16
    spot, lane = lax.axis_index("sp"), lax.axis_index("tp")
    depth = groups // width
    z, y = lax.div(spot, width), lax.rem(spot, width)
    core = lax.rem(lane, 2)
    core_peer = lane + 1 - 2 * core
    far_peer = lax.rem(lane + lanes // 2, lanes)
    mate = spot + 1 - 2 * y
    token_count, model_width = normed.shape
    quarter = model_width // lanes
    half = model_width // 2
    span = rows.shape[1]
    given = (normed, cots)
    laid = (rows, row_cots)

    def columns(who, size):
        return pl.ds(pl.multiple_of(who * size, size), size)

    def part(ref, block, who):
        return ref.at[block, :, columns(who, quarter)]

    def source(side, level):
        return z + level * (2 * side - 1)

    def valid(side, level):
        at = source(side, level)
        return jnp.logical_and(level > 0, jnp.logical_and(at >= 0, at < depth))

    def present(side, level, line):
        near = jnp.logical_and(side == 0, line == level + 1)
        return jnp.logical_or(valid(side, level), jnp.logical_and(level <= 0, near))

    def onward(side):
        at = z + 1 - 2 * side
        return jnp.logical_and(at >= 0, at < depth)

    def block_of(side, level, line):
        at = source(side, lax.max(level, 0))
        return at * width + lax.rem(y + line, width)

    def tell(offset):
        goal = lax.rem(spot + offset, groups)
        return remote(info, infos.at[spot], send_i.at[offset], recv_i.at[spot], sp=goal)

    def told(offset):
        origin = lax.rem(spot - offset + groups, groups)
        return remote(info, infos.at[origin], send_i.at[offset], recv_i.at[origin], sp=origin)

    def is_end(at):
        return jnp.logical_or(at == 0, at == depth - 1)

    def end_of(at):
        return lax.min(at, 1)

    def by_kind(at, wide, narrow):
        @pl.when(is_end(at))
        def _():
            wide()

        @pl.when(jnp.logical_not(is_end(at)))
        def _():
            narrow()

    def hop_wide(k, at, side, own):
        held = dense_wide.at[k, end_of(at)]
        return remote(
            given[k].at[:, columns(core, half)] if own else held,
            held,
            send_z.at[k, side, at],
            recv_z.at[k, at],
            sp=spot + width * (1 - 2 * side),
        )

    def over_wide(k, at):
        return remote(
            to_mate_wide.at[k, end_of(at)],
            laid[k].at[at * width + y, :, columns(core, half)],
            send_y.at[k, at],
            recv_y.at[k, at],
            sp=mate,
        )

    def hop(k, at, side, own):
        held = dense.at[k, at]
        return remote(
            given[k].at[:, columns(lane, quarter)] if own else held,
            held,
            send_z.at[k, side, at],
            recv_z.at[k, at],
            sp=spot + width * (1 - 2 * side),
        )

    def over(k, at):
        return remote(
            to_mate.at[k, at],
            part(laid[k], at * width + y, lane),
            send_y.at[k, at],
            recv_y.at[k, at],
            sp=mate,
        )

    def over_own(k):
        return remote(
            to_mate_own.at[k],
            laid[k].at[spot, :, columns(core, half)],
            send_o.at[k],
            recv_o.at[k],
            sp=mate,
        )

    def far_copy(k, block):
        held = part(laid[k], block, lane)
        return remote(held, held, send_x.at[k, block], recv_x.at[k, block], tp=far_peer)

    def core_copy(k, block):
        held = part(laid[k], block, lane)
        return remote(held, held, send_c.at[k, block], recv_c.at[k, block], tp=core_peer)

    def half_copy(k, block):
        held = laid[k].at[block, :, columns(core, half)]
        return remote(held, held, send_c.at[k, block], recv_c.at[k, block], tp=core_peer)

    def pass_copy(k, block):
        held = part(laid[k], block, far_peer)
        return remote(held, held, send_f.at[k, block], recv_f.at[k, block], tp=core_peer)

    def to_core(block, far):
        who = lax.rem(core_peer + far * (lanes // 2), lanes)
        return remote(
            part(partial, block, who),
            from_core.at[block, far],
            send_t.at[block, far],
            recv_t.at[block, far],
            tp=core_peer,
        )

    def to_far_peer(block):
        return remote(
            to_far.at[block],
            from_far.at[block],
            send_r.at[block],
            recv_r.at[block],
            tp=far_peer,
        )

    def home(block):
        return remote(
            summed.at[block], returned.at[spot], send_h.at[block], recv_h.at[spot], sp=block
        )

    def home_from(block):
        return remote(
            summed.at[block], returned.at[block], send_h.at[block], recv_h.at[block], sp=block
        )

    def matches(block, expert):
        slot = lax.broadcasted_iota(jnp.int32, (span, token_count), 0) + expert * span
        slot = slot.astype(f32)
        return slot == infos[block, 0:1, :], slot == infos[block, 1:2, :]

    def chosen(block, expert):
        first, second = matches(block, expert)
        return jnp.where(jnp.logical_or(first, second), 1.0, 0.0).astype(bf16)

    def weights_of(block):
        first, second = matches(block, spot)
        return jnp.sum(
            jnp.where(first, infos[block, 2:3, :], 0.0)
            + jnp.where(second, infos[block, 3:4, :], 0.0),
            axis=1,
            keepdims=True,
        )

    def placed(matrix, values):
        return jnp.dot(matrix, values, preferred_element_type=f32).astype(bf16)

    def both(body):
        def step(side, carry):
            body(side)
            return carry

        lax.fori_loop(0, 2, step, 0)

    def each_block(level, body):
        def step(at, carry):
            side, line = lax.div(at, 2), lax.rem(at, 2)

            @pl.when(present(side, level, line))
            def _():
                body(block_of(side, level, line), side, line)

            return carry

        lax.fori_loop(0, 4, step, 0)

    core_side, far_side = core_peer, far_peer
    greet(groups, spot, core_side, far_side)

    def tell_all(offset, carry):
        tell(offset).start()
        return carry

    lax.fori_loop(1, groups, tell_all, 0)
    for k in (0, 1):
        for side in (0, 1):

            @pl.when(onward(side))
            def _():
                by_kind(
                    z,
                    lambda: hop_wide(k, z, side, True).start(),
                    lambda: hop(k, z, side, True).start(),
                )

    infos[spot] = info[...]
    mine_there = chosen(spot, mate)
    for k in (0, 1):
        to_mate_own[k] = placed(mine_there, given[k][:, columns(core, half)])
        over_own(k).start()
    mine_here = chosen(spot, spot)

    def lay_own(at, carry):
        for k in (0, 1):
            laid[k][spot, :, columns(at, quarter)] = placed(
                mine_here, given[k][:, columns(at, quarter)]
            )
        return carry

    lax.fori_loop(0, lanes, lay_own, 0)

    def move(copy, k, at, side):
        copy(k, at, side, False).wait_recv()

        @pl.when(onward(side))
        def _():
            copy(k, at, side, False).start()

    def at_ends(level, ends, body):
        def step(side):
            at = source(side, level)
            kind = is_end(at) if ends else jnp.logical_not(is_end(at))

            @pl.when(jnp.logical_and(valid(side, level), kind))
            def _():
                body(side, at, at * width + y)

        both(step)

    def early(side, level):
        return jnp.logical_and(onward(side), level >= 2)

    def take_narrow(level, k):
        def body(side, at, block):
            move(hop, k, at, side)
            values = dense[k, at]
            laid[k][block, :, columns(lane, quarter)] = placed(chosen(block, spot), values)
            far_copy(k, block).start()
            core_copy(k, block).start()
            to_mate[k, at] = placed(chosen(block, mate), values)
            over(k, at).start()

        at_ends(level, False, body)

    def move_early(level, k):
        def body(side, at, block):
            @pl.when(early(side, level))
            def _():
                move(hop_wide, k, at, side)

        at_ends(level, True, body)

    def take_wide(level, k):
        def body(side, at, block):
            @pl.when(jnp.logical_not(early(side, level)))
            def _():
                move(hop_wide, k, at, side)

            end = end_of(at)
            values = dense_wide[k, end]
            to_mate_wide[k, end] = placed(chosen(block, mate), values)
            over_wide(k, at).start()
            laid[k][block, :, columns(core, half)] = placed(chosen(block, spot), values)
            half_copy(k, block).start()

        at_ends(level, True, body)

    def receive_level(level, k):
        def receive(side):
            @pl.when(valid(side, level))
            def _():
                at = source(side, level)
                block = at * width + 1 - y

                def wide():
                    over_wide(k, at).wait_recv()
                    half_copy(k, block).start()

                def narrow():
                    over(k, at).wait_recv()
                    far_copy(k, block).start()
                    core_copy(k, block).start()

                by_kind(at, wide, narrow)

        both(receive)

    def share_level(level):
        @pl.when(level == 0)
        def _():
            for k in (0, 1):
                over_own(k).wait_recv()
                half_copy(k, mate).start()

        def share(block, side, line):
            narrow = jnp.logical_not(is_end(source(side, level)))

            @pl.when(jnp.logical_and(level > 0, narrow))
            def _():
                for k in (0, 1):
                    far_copy(k, block).wait_recv()
                    pass_copy(k, block).start()

        each_block(level, share)

    def compute_level(level):
        def compute(block, side, line):
            @pl.when(level > 0)
            def _():
                def wide():
                    for k in (0, 1):
                        half_copy(k, block).wait_recv()

                def narrow():
                    for k in (0, 1):
                        core_copy(k, block).wait_recv()
                        pass_copy(k, block).wait_recv()

                by_kind(source(side, level), wide, narrow)

            @pl.when(jnp.logical_and(level == 0, line == 1))
            def _():
                for k in (0, 1):
                    half_copy(k, mate).wait_recv()

            weight = weights_of(block)
            entry_rows = rows[block]
            gate_pre = jnp.dot(entry_rows, gate_mat[...], preferred_element_type=f32)
            up_pre = jnp.dot(entry_rows, up_mat[...], preferred_element_type=f32)
            pulled = lax.dot_general(
                row_cots[block],
                down_mat[...],
                (((1,), (1,)), ((), ())),
                preferred_element_type=f32,
            )
            logistic = jax.nn.sigmoid(gate_pre)
            activated = gate_pre * logistic
            hidden[block] = (activated * up_pre * weight).astype(bf16)
            dhidden = pulled * weight
            grad_gate = (
                dhidden * up_pre * logistic * (1.0 + gate_pre * (1.0 - logistic))
            ).astype(bf16)
            grad_up = (dhidden * activated).astype(bf16)
            dgate[block] = grad_gate
            dup[block] = grad_up

            def back(at, carry):
                picked = columns(at, quarter)
                over_width = (((1,), (1,)), ((), ()))
                partial[block, :, picked] = (
                    lax.dot_general(
                        grad_gate, gate_mat[picked, :], over_width, preferred_element_type=f32
                    )
                    + lax.dot_general(
                        grad_up, up_mat[picked, :], over_width, preferred_element_type=f32
                    )
                ).astype(bf16)
                return carry

            lax.fori_loop(0, lanes, back, 0)
            to_core(block, 1).start()
            to_core(block, 0).start()

        each_block(level, compute)

    def middle_level(level):
        def middle(block, side, line):
            to_core(block, 1).wait_recv()
            to_far[block] = (
                partial[block, :, columns(far_peer, quarter)].astype(f32)
                + from_core[block, 1].astype(f32)
            ).astype(bf16)
            to_far_peer(block).start()

        each_block(level, middle)

    def total_level(level):
        def total(block, side, line):
            to_core(block, 0).wait_recv()
            to_far_peer(block).wait_recv()
            value = (
                partial[block, :, columns(lane, quarter)].astype(f32)
                + from_core[block, 0].astype(f32)
                + from_far[block].astype(f32)
            ).astype(bf16)

            @pl.when(block == spot)
            def _():
                returned[spot] = value

            @pl.when(block != spot)
            def _():
                summed[block] = value
                home(block).start()

        each_block(level, total)

    def weight_grads():
        slots = groups * span
        down_in = (((0,), (0,)), ((), ()))

        def down_step(at, carry):
            picked = columns(at, quarter)
            grad_b[:, picked] = lax.dot_general(
                hidden[...].reshape(slots, hidden.shape[2]),
                row_cots[:, :, picked].reshape(slots, quarter),
                down_in,
                preferred_element_type=f32,
            )
            return carry

        lax.fori_loop(0, lanes, down_step, 0)
        down_copy = pltpu.make_async_copy(grad_b, down_out, local_sem.at[0])
        down_copy.start()
        copies = [down_copy]
        for spread, out, index in ((dgate, gate_out, 0), (dup, up_out, 1)):

            def step(at, carry):
                picked = columns(at, quarter)
                grad_a[index, picked, :] = lax.dot_general(
                    rows[:, :, picked].reshape(slots, quarter),
                    spread[...].reshape(slots, spread.shape[2]),
                    down_in,
                    preferred_element_type=f32,
                )
                return carry

            lax.fori_loop(0, lanes, step, 0)
            copy = pltpu.make_async_copy(grad_a.at[index], out, local_sem.at[index + 1])
            copy.start()
            copies.append(copy)
        for copy in copies:
            copy.wait()

    def advance(level, carry):
        @pl.when(level == 1)
        def _():
            def hear_all(offset, carry):
                told(offset).wait_recv()
                return carry

            lax.fori_loop(1, groups, hear_all, 0)

        take_narrow(level, 0)
        take_narrow(level, 1)
        take_wide(level, 0)
        share_level(level - 1)
        move_early(level, 1)
        compute_level(level - 1)
        middle_level(level - 1)
        take_wide(level, 1)
        move_early(level + 1, 0)
        receive_level(level, 0)

        @pl.when(level < depth)
        def _():
            total_level(level - 1)

        receive_level(level, 1)
        return carry

    lax.fori_loop(0, depth + 1, advance, 0)
    weight_grads()
    total_level(depth - 1)
    combined[...] = jnp.zeros_like(combined)

    def combine_level(level, carry):
        def combine(block, side, line):
            @pl.when(block != spot)
            def _():
                home_from(block).wait_recv()

            slot = lax.broadcasted_iota(jnp.int32, (token_count, span), 1) + block * span
            slot = slot.astype(f32)
            hit = jnp.logical_or(slot == targets[:, 0:1], slot == targets[:, 1:2])
            picked = jnp.where(hit, 1.0, 0.0).astype(bf16)
            combined[...] += jnp.dot(picked, returned[block], preferred_element_type=f32)

        each_block(level, combine)
        return carry

    lax.fori_loop(-1, depth, combine_level, 0)

    def gather_part(who):
        return gathered.at[:, columns(who, quarter)]

    def gather_copy(index, who, peer):
        held = gather_part(who)
        return remote(held, held, send_g.at[index], recv_g.at[index], tp=peer)

    gathered[:, columns(lane, quarter)] = combined[...].astype(bf16)
    gather_copy(0, lane, far_peer).start()
    gather_copy(1, lane, core_peer).start()
    gather_copy(0, lane, far_peer).wait_recv()
    gather_copy(2, far_peer, core_peer).start()
    gather_copy(0, lane, far_peer).wait_send()
    gather_copy(1, lane, core_peer).wait()
    gather_copy(2, far_peer, core_peer).wait()

    def finish_info(offset, carry):
        tell(offset).wait_send()
        origin = lax.rem(spot + offset, groups)
        home_from(origin).wait_send()
        return carry

    lax.fori_loop(1, groups, finish_info, 0)
    for k in (0, 1):
        for side in (0, 1):

            @pl.when(onward(side))
            def _():
                by_kind(
                    z,
                    lambda: hop_wide(k, z, side, True).wait_send(),
                    lambda: hop(k, z, side, True).wait_send(),
                )

        over_own(k).wait_send()
        half_copy(k, mate).wait_send()

    def finish_level(level, carry):
        def finish(block, side, line):
            to_core(block, 0).wait_send()
            to_core(block, 1).wait_send()
            to_far_peer(block).wait_send()

            @pl.when(level > 0)
            def _():
                at = source(side, level)

                def done(hold, cross):
                    @pl.when(line == 0)
                    def _():
                        for k in (0, 1):
                            cross(k, at).wait_send()

                            @pl.when(onward(side))
                            def _():
                                hold(k, at, side, False).wait_send()

                def wide():
                    for k in (0, 1):
                        half_copy(k, block).wait_send()
                    done(hop_wide, over_wide)

                def narrow():
                    for k in (0, 1):
                        far_copy(k, block).wait_send()
                        core_copy(k, block).wait_send()
                        pass_copy(k, block).wait_send()
                    done(hop, over)

                by_kind(at, wide, narrow)

        each_block(level, finish)
        return carry

    lax.fori_loop(-1, depth, finish_level, 0)


def experts(normed, cots, info, targets, gate_mat, up_mat, down_mat, groups, lanes, span):
    token_count, model_width = normed.shape
    inner = gate_mat.shape[1]
    quarter = model_width // lanes
    width = 2
    depth = groups // width
    bf16, f32 = jnp.bfloat16, jnp.float32
    dma = pltpu.SemaphoreType.DMA
    inside = pl.BlockSpec(memory_space=pltpu.VMEM)
    anywhere = pl.BlockSpec(memory_space=pl.ANY)
    block = (groups, span, quarter)
    whole = (groups, span, model_width)
    thin = (groups, span, inner)
    vmem = pltpu.VMEM
    return pl.pallas_call(
        functools.partial(expert_kernel, groups, width, lanes),
        out_shape=(
            jax.ShapeDtypeStruct(normed.shape, bf16),
            jax.ShapeDtypeStruct(gate_mat.shape, f32),
            jax.ShapeDtypeStruct(up_mat.shape, f32),
            jax.ShapeDtypeStruct(down_mat.shape, f32),
        ),
        in_specs=[inside] * 7,
        out_specs=(inside, anywhere, anywhere, anywhere),
        scratch_shapes=[
            vmem((groups,) + info.shape, f32),
            vmem((2, depth, token_count, quarter), bf16),
            vmem((2, 2, token_count, model_width // 2), bf16),
            vmem((2, depth, span, quarter), bf16),
            vmem((2, 2, span, model_width // 2), bf16),
            vmem((2, span, model_width // 2), bf16),
            vmem(whole, bf16),
            vmem(whole, bf16),
            vmem(thin, bf16),
            vmem(thin, bf16),
            vmem(thin, bf16),
            vmem(whole, bf16),
            vmem((groups, 2, span, quarter), bf16),
            vmem(block, bf16),
            vmem(block, bf16),
            vmem(block, bf16),
            vmem(block, bf16),
            vmem((token_count, quarter), f32),
            vmem((2,) + gate_mat.shape, f32),
            vmem(down_mat.shape, f32),
            dma((3,)),
            dma((groups,)),
            dma((groups,)),
            dma((2, 2, depth)),
            dma((2, depth)),
            dma((2, depth)),
            dma((2, depth)),
            dma((2,)),
            dma((2,)),
        ]
        + [dma((2, groups))] * 6
        + [dma((groups, 2))] * 2
        + [dma((groups,))] * 4
        + [dma((3,))] * 2,
        compiler_params=pltpu.CompilerParams(
            collective_id=1, has_side_effects=True, vmem_limit_bytes=63 * 2**20
        ),
        cost_estimate=pl.CostEstimate(
            flops=16 * groups * span * model_width * inner,
            bytes_accessed=150 * 2**20,
            transcendentals=0,
        ),
        name="experts",
    )(normed, cots, info, targets, gate_mat, up_mat, down_mat)


def reduce_kernel(groups, lanes, partial, total, arrived, send_sems, recv_sems):
    f32 = jnp.float32
    spot, lane = lax.axis_index("sp"), lax.axis_index("tp")
    core_peer = lane + 1 - 2 * lax.rem(lane, 2)
    far_peer = lax.rem(lane + lanes // 2, lanes)

    def across(offset):
        goal = lax.rem(spot + offset, groups)
        return remote(
            partial.at[goal],
            arrived.at[offset],
            send_sems.at[offset],
            recv_sems.at[offset],
            sp=goal,
        )

    greet(groups, spot, core_peer, far_peer)

    def launch(offset, carry):
        across(offset).start()
        return carry

    lax.fori_loop(1, groups, launch, 0)
    total[...] = partial[spot].astype(f32)

    def add(offset, carry):
        across(offset).wait_recv()
        total[...] += arrived[offset].astype(f32)
        return carry

    lax.fori_loop(1, groups, add, 0)

    def finish(offset, carry):
        across(offset).wait_send()
        return carry

    lax.fori_loop(1, groups, finish, 0)


def reduce_rows(partial, groups, lanes):
    sem = pltpu.SemaphoreType.DMA
    inside = pl.BlockSpec(memory_space=pltpu.VMEM)
    return pl.pallas_call(
        functools.partial(reduce_kernel, groups, lanes),
        out_shape=jax.ShapeDtypeStruct(partial.shape[1:], jnp.float32),
        in_specs=[inside],
        out_specs=inside,
        scratch_shapes=[
            pltpu.VMEM(partial.shape, partial.dtype),
            sem((groups,)),
            sem((groups,)),
        ],
        compiler_params=pltpu.CompilerParams(collective_id=4, has_side_effects=True),
        name="reduce_rows",
    )(partial)


def on_device(
    resid_in,
    cotangent,
    norm_gain,
    routes,
    route_weights,
    gate_weight,
    up_weight,
    down_weight,
    out_weight,
    gate_b,
    gate_c,
    values_u,
    taps,
):
    f32 = jnp.float32
    bf16 = jnp.bfloat16
    token_count, model_width = resid_in.shape
    groups = lax.axis_size("sp")
    lanes = lax.axis_size("tp")
    local_experts = gate_weight.shape[0]
    expert_total = local_experts * groups
    capacity = 4 * token_count // expert_total
    slot_span = local_experts * capacity
    resid_wide = resid_in.astype(f32)
    inv_rms = lax.rsqrt(jnp.mean(resid_wide * resid_wide, axis=1, keepdims=True) + norm_eps)
    normed = (resid_wide * inv_rms * norm_gain).astype(bf16)
    mixed = gate_c.astype(f32) * values_u.astype(f32)
    earlier = passed_along(mixed[-2:], "sp", 1)
    names = jnp.arange(expert_total, dtype=jnp.int32)
    chosen = routes[:, :, None] == names[None, None, :]
    named = jnp.any(chosen, axis=1).astype(bf16)
    order = jnp.arange(token_count, dtype=jnp.int32)
    strict = (order[:, None] > order[None, :]).astype(bf16)
    before = jnp.dot(strict, named, preferred_element_type=f32).astype(jnp.int32)
    rank = jnp.sum(jnp.where(chosen, before[:, None, :], 0), axis=2)
    targets = routes * capacity + rank
    info = jnp.concatenate(
        [
            targets.T.astype(f32),
            route_weights.T,
            jnp.zeros((4, token_count), f32),
        ],
        axis=0,
    )
    gathered, grad_gate, grad_up, grad_down = experts(
        normed,
        cotangent,
        info,
        targets.astype(f32),
        gate_weight[0],
        up_weight[0],
        down_weight[0],
        groups,
        lanes,
        slot_span,
    )
    dnormed = gathered.astype(f32)
    scaled = dnormed * norm_gain
    resid_grad = (
        cotangent.astype(f32)
        + inv_rms * scaled
        - resid_wide * inv_rms**3 * jnp.mean(scaled * resid_wide, axis=1, keepdims=True)
    )
    grad_resid = resid_grad.astype(bf16)
    extended = jnp.concatenate([earlier, mixed], axis=0)
    conv = (
        taps[0] * extended[:token_count]
        + taps[1] * extended[1 : token_count + 1]
        + taps[2] * extended[2 : token_count + 2]
    )
    merged = (gate_b.astype(f32) * conv).astype(bf16)
    out_partial = jnp.einsum("td,tc->dc", grad_resid, merged, preferred_element_type=f32)
    grad_out_weight = reduce_rows(
        out_partial.astype(bf16).reshape(groups, model_width // groups, merged.shape[1]),
        groups,
        lanes,
    )
    dmerged = jnp.dot(grad_resid, out_weight, preferred_element_type=f32)
    grad_gate_b = (dmerged * conv).astype(bf16)
    dconv = dmerged * gate_b.astype(f32)
    later = passed_along(dconv[:2], "sp", -1)
    extended_grad = jnp.concatenate([dconv, later], axis=0)
    dmixed = (
        taps[2] * extended_grad[:token_count]
        + taps[1] * extended_grad[1 : token_count + 1]
        + taps[0] * extended_grad[2 : token_count + 2]
    )
    grad_gate_c = (dmixed * values_u.astype(f32)).astype(bf16)
    grad_values = (dmixed * gate_c.astype(f32)).astype(bf16)
    return (
        grad_gate[None],
        grad_up[None],
        grad_down[None],
        grad_resid,
        grad_out_weight,
        grad_gate_b,
        grad_gate_c,
        grad_values,
    )


def solution(mesh):
    placed = (
        P("sp", None),
        P("sp", None),
        P(),
        P("sp", None),
        P("sp", None),
        P("sp", None, "tp"),
        P("sp", None, "tp"),
        P("sp", "tp", None),
        P(None, "tp"),
        P("sp", "tp"),
        P("sp", "tp"),
        P("sp", "tp"),
        P(None, "tp"),
    )
    return jax.shard_map(
        on_device,
        mesh=mesh,
        in_specs=placed,
        out_specs=(
            P("sp", None, "tp"),
            P("sp", None, "tp"),
            P("sp", "tp", None),
            P("sp", None),
            P("sp", "tp"),
            P("sp", "tp"),
            P("sp", "tp"),
            P("sp", "tp"),
        ),
        check_vma=False,
    )
```

```python
import functools

import jax
import jax.numpy as jnp
from jax import lax
from jax.experimental import pallas as pl
from jax.experimental.pallas import tpu as pltpu
from jax.sharding import PartitionSpec as P

norm_eps = 1e-06


def remote(source, target, send_sem, recv_sem, **device):
    return pltpu.make_async_remote_copy(
        src_ref=source,
        dst_ref=target,
        send_sem=send_sem,
        recv_sem=recv_sem,
        device_id=device,
        device_id_type=pl.DeviceIdType.MESH,
    )


def greet(groups, spot, core_peer, far_peer):
    barrier = pltpu.get_barrier_semaphore()

    def to_group(offset, carry):
        pl.semaphore_signal(
            barrier,
            inc=1,
            device_id={"sp": lax.rem(spot + offset, groups)},
            device_id_type=pl.DeviceIdType.MESH,
        )
        return carry

    lax.fori_loop(1, groups, to_group, 0)
    for peer in (core_peer, far_peer):
        pl.semaphore_signal(
            barrier, inc=1, device_id={"tp": peer}, device_id_type=pl.DeviceIdType.MESH
        )
    pl.semaphore_wait(barrier, groups + 1)


def expert_kernel(
    groups,
    width,
    lanes,
    resid,
    cots,
    gain,
    edge,
    info,
    targets,
    gate_mat,
    up_mat,
    down_mat,
    resid_grad,
    edge_got,
    gate_out,
    up_out,
    down_out,
    normed,
    inverse,
    product,
    gathered,
    infos,
    dense,
    dense_wide,
    to_mate,
    to_mate_wide,
    to_mate_own,
    rows,
    row_cots,
    hidden,
    dgate,
    dup,
    partial,
    from_core,
    to_far,
    from_far,
    returned,
    combined,
    grad_a,
    grad_b,
    local_sem,
    send_i,
    recv_i,
    send_z,
    recv_z,
    send_y,
    recv_y,
    send_o,
    recv_o,
    send_x,
    recv_x,
    send_c,
    recv_c,
    send_f,
    recv_f,
    send_t,
    recv_t,
    send_r,
    recv_r,
    send_h,
    recv_h,
    send_g,
    recv_g,
    send_e,
    recv_e,
):
    f32 = jnp.float32
    bf16 = jnp.bfloat16
    spot, lane = lax.axis_index("sp"), lax.axis_index("tp")
    depth = groups // width
    z, y = lax.div(spot, width), lax.rem(spot, width)
    core = lax.rem(lane, 2)
    core_peer = lane + 1 - 2 * core
    far_peer = lax.rem(lane + lanes // 2, lanes)
    mate = spot + 1 - 2 * y
    token_count, model_width = resid.shape
    quarter = model_width // lanes
    half = model_width // 2
    span = rows.shape[1]
    strip = 16
    tall = 64
    given = (normed, cots)
    laid = (rows, row_cots)

    def columns(who, size):
        return pl.ds(pl.multiple_of(who * size, size), size)

    def part(ref, block, who):
        return ref.at[block, :, columns(who, quarter)]

    def source(side, level):
        return z + level * (2 * side - 1)

    def valid(side, level):
        at = source(side, level)
        return jnp.logical_and(level > 0, jnp.logical_and(at >= 0, at < depth))

    def present(side, level, line):
        near = jnp.logical_and(side == 0, line == level + 1)
        return jnp.logical_or(valid(side, level), jnp.logical_and(level <= 0, near))

    def onward(side):
        at = z + 1 - 2 * side
        return jnp.logical_and(at >= 0, at < depth)

    def block_of(side, level, line):
        at = source(side, lax.max(level, 0))
        return at * width + lax.rem(y + line, width)

    def tell(offset):
        goal = lax.rem(spot + offset, groups)
        return remote(info, infos.at[spot], send_i.at[offset], recv_i.at[spot], sp=goal)

    def told(offset):
        origin = lax.rem(spot - offset + groups, groups)
        return remote(info, infos.at[origin], send_i.at[offset], recv_i.at[origin], sp=origin)

    def is_end(at):
        return jnp.logical_or(at == 0, at == depth - 1)

    def end_of(at):
        return lax.min(at, 1)

    def by_kind(at, wide, narrow):
        @pl.when(is_end(at))
        def _():
            wide()

        @pl.when(jnp.logical_not(is_end(at)))
        def _():
            narrow()

    def hop_wide(k, at, side, own):
        held = dense_wide.at[k, end_of(at)]
        return remote(
            given[k].at[:, columns(core, half)] if own else held,
            held,
            send_z.at[k, side, at],
            recv_z.at[k, at],
            sp=spot + width * (1 - 2 * side),
        )

    def over_wide(k, at):
        return remote(
            to_mate_wide.at[k, end_of(at)],
            laid[k].at[at * width + y, :, columns(core, half)],
            send_y.at[k, at],
            recv_y.at[k, at],
            sp=mate,
        )

    def hop(k, at, side, own):
        held = dense.at[k, at]
        return remote(
            given[k].at[:, columns(lane, quarter)] if own else held,
            held,
            send_z.at[k, side, at],
            recv_z.at[k, at],
            sp=spot + width * (1 - 2 * side),
        )

    def over(k, at):
        return remote(
            to_mate.at[k, at],
            part(laid[k], at * width + y, lane),
            send_y.at[k, at],
            recv_y.at[k, at],
            sp=mate,
        )

    def over_own(k):
        return remote(
            to_mate_own.at[k],
            laid[k].at[spot, :, columns(core, half)],
            send_o.at[k],
            recv_o.at[k],
            sp=mate,
        )

    def far_copy(k, block):
        held = part(laid[k], block, lane)
        return remote(held, held, send_x.at[k, block], recv_x.at[k, block], tp=far_peer)

    def core_copy(k, block):
        held = part(laid[k], block, lane)
        return remote(held, held, send_c.at[k, block], recv_c.at[k, block], tp=core_peer)

    def half_copy(k, block):
        held = laid[k].at[block, :, columns(core, half)]
        return remote(held, held, send_c.at[k, block], recv_c.at[k, block], tp=core_peer)

    def pass_copy(k, block):
        held = part(laid[k], block, far_peer)
        return remote(held, held, send_f.at[k, block], recv_f.at[k, block], tp=core_peer)

    def to_core(block, far):
        who = lax.rem(core_peer + far * (lanes // 2), lanes)
        return remote(
            part(partial, block, who),
            from_core.at[block, far],
            send_t.at[block, far],
            recv_t.at[block, far],
            tp=core_peer,
        )

    def to_far_peer(block):
        return remote(
            to_far.at[block],
            from_far.at[block],
            send_r.at[block],
            recv_r.at[block],
            tp=far_peer,
        )

    def home(block):
        return remote(
            from_far.at[block], returned.at[spot], send_h.at[block], recv_h.at[spot], sp=block
        )

    def home_from(block):
        return remote(
            from_far.at[block], returned.at[block], send_h.at[block], recv_h.at[block], sp=block
        )

    def matches(block, expert):
        slot = lax.broadcasted_iota(jnp.int32, (span, token_count), 0) + expert * span
        slot = slot.astype(f32)
        return slot == infos[block, 0:1, :], slot == infos[block, 1:2, :]

    def chosen(block, expert):
        first, second = matches(block, expert)
        return jnp.where(jnp.logical_or(first, second), 1.0, 0.0).astype(bf16)

    def weights_of(block):
        first, second = matches(block, spot)
        return jnp.sum(
            jnp.where(first, infos[block, 2:3, :], 0.0)
            + jnp.where(second, infos[block, 3:4, :], 0.0),
            axis=1,
            keepdims=True,
        )

    def placed(matrix, values):
        return jnp.dot(matrix, values, preferred_element_type=f32).astype(bf16)

    def both(body):
        def step(side, carry):
            body(side)
            return carry

        lax.fori_loop(0, 2, step, 0)

    def each_block(level, body):
        def step(at, carry):
            side, line = lax.div(at, 2), lax.rem(at, 2)

            @pl.when(present(side, level, line))
            def _():
                body(block_of(side, level, line), side, line)

            return carry

        lax.fori_loop(0, 4, step, 0)

    core_side, far_side = core_peer, far_peer
    greet(groups, spot, core_side, far_side)

    def tell_all(offset, carry):
        tell(offset).start()
        return carry

    lax.fori_loop(1, groups, tell_all, 0)
    def shift():
        return remote(
            edge, edge_got, send_e.at[0], recv_e.at[0], sp=lax.rem(spot + 1, groups)
        )

    @pl.when(spot < groups - 1)
    def _():
        shift().start()

    @pl.when(spot == 0)
    def _():
        edge_got[...] = jnp.zeros_like(edge_got)

    def send_own(k):
        for side in (0, 1):

            @pl.when(onward(side))
            def _():
                by_kind(
                    z,
                    lambda: hop_wide(k, z, side, True).start(),
                    lambda: hop(k, z, side, True).start(),
                )

    send_own(1)

    def norm_strip(at, carry):
        picked = pl.ds(pl.multiple_of(at * strip, strip), strip)
        wide = resid[picked, :].astype(f32)
        mean = jnp.sum(wide * wide, axis=1, keepdims=True) * (1.0 / model_width)
        scale = lax.rsqrt(mean + norm_eps)
        inverse[picked, :] = scale
        normed[picked, :] = (wide * scale * gain[...]).astype(bf16)
        return carry

    lax.fori_loop(0, token_count // strip, norm_strip, 0, unroll=2)
    send_own(0)
    infos[spot] = info[...]
    mine_there = chosen(spot, mate)
    for k in (1, 0):
        to_mate_own[k] = placed(mine_there, given[k][:, columns(core, half)])
        over_own(k).start()
    mine_here = chosen(spot, spot)

    def lay_own(at, carry):
        for k in (0, 1):
            laid[k][spot, :, columns(at, quarter)] = placed(
                mine_here, given[k][:, columns(at, quarter)]
            )
        return carry

    lax.fori_loop(0, lanes, lay_own, 0)

    def move(copy, k, at, side):
        copy(k, at, side, False).wait_recv()

        @pl.when(onward(side))
        def _():
            copy(k, at, side, False).start()

    def at_ends(level, ends, body):
        def step(side):
            at = source(side, level)
            kind = is_end(at) if ends else jnp.logical_not(is_end(at))

            @pl.when(jnp.logical_and(valid(side, level), kind))
            def _():
                body(side, at, at * width + y)

        both(step)

    def early(side, level):
        return jnp.logical_and(onward(side), level >= 2)

    def take_narrow(level, k):
        def body(side, at, block):
            move(hop, k, at, side)
            values = dense[k, at]
            laid[k][block, :, columns(lane, quarter)] = placed(chosen(block, spot), values)
            far_copy(k, block).start()
            core_copy(k, block).start()
            to_mate[k, at] = placed(chosen(block, mate), values)
            over(k, at).start()

        at_ends(level, False, body)

    def move_early(level, k):
        def body(side, at, block):
            @pl.when(early(side, level))
            def _():
                move(hop_wide, k, at, side)

        at_ends(level, True, body)

    def take_wide(level, k):
        def body(side, at, block):
            @pl.when(jnp.logical_not(early(side, level)))
            def _():
                move(hop_wide, k, at, side)

            end = end_of(at)
            values = dense_wide[k, end]
            to_mate_wide[k, end] = placed(chosen(block, mate), values)
            over_wide(k, at).start()
            laid[k][block, :, columns(core, half)] = placed(chosen(block, spot), values)
            half_copy(k, block).start()

        at_ends(level, True, body)

    def receive_level(level, k):
        def receive(side):
            @pl.when(valid(side, level))
            def _():
                at = source(side, level)
                block = at * width + 1 - y

                def wide():
                    over_wide(k, at).wait_recv()
                    half_copy(k, block).start()

                def narrow():
                    over(k, at).wait_recv()
                    far_copy(k, block).start()
                    core_copy(k, block).start()

                by_kind(at, wide, narrow)

        both(receive)

    def share_level(level):
        @pl.when(level == 0)
        def _():
            for k in (0, 1):
                over_own(k).wait_recv()
                half_copy(k, mate).start()

        def share(block, side, line):
            narrow = jnp.logical_not(is_end(source(side, level)))

            @pl.when(jnp.logical_and(level > 0, narrow))
            def _():
                for k in (0, 1):
                    far_copy(k, block).wait_recv()
                    pass_copy(k, block).start()

        each_block(level, share)

    def ahead(level, side, line):
        return jnp.logical_and(
            jnp.logical_and(level > 0, line == 0), is_end(source(side, level))
        )

    def work_level(level, first):
        def chosen_now(block, side, line, body):
            now = ahead(level, side, line)

            @pl.when(now if first else jnp.logical_not(now))
            def _():
                body(block, side, line)

        compute_level(level, chosen_now)
        middle_level(level, chosen_now)

    def compute_level(level, chosen_now):
        def compute(block, side, line):
            @pl.when(level > 0)
            def _():
                def wide():
                    for k in (0, 1):
                        half_copy(k, block).wait_recv()

                def narrow():
                    for k in (0, 1):
                        core_copy(k, block).wait_recv()
                        pass_copy(k, block).wait_recv()

                by_kind(source(side, level), wide, narrow)

            @pl.when(jnp.logical_and(level == 0, line == 1))
            def _():
                for k in (0, 1):
                    half_copy(k, mate).wait_recv()

            weight = weights_of(block)
            entry_rows = rows[block]
            gate_pre = jnp.dot(entry_rows, gate_mat[...], preferred_element_type=f32)
            up_pre = jnp.dot(entry_rows, up_mat[...], preferred_element_type=f32)
            pulled = lax.dot_general(
                row_cots[block],
                down_mat[...],
                (((1,), (1,)), ((), ())),
                preferred_element_type=f32,
            )
            logistic = jax.nn.sigmoid(gate_pre)
            activated = gate_pre * logistic
            hidden[block] = (activated * up_pre * weight).astype(bf16)
            dhidden = pulled * weight
            grad_gate = (
                dhidden * up_pre * logistic * (1.0 + gate_pre * (1.0 - logistic))
            ).astype(bf16)
            grad_up = (dhidden * activated).astype(bf16)
            dgate[block] = grad_gate
            dup[block] = grad_up

            def back(at, carry):
                picked = columns(at, quarter)
                over_width = (((1,), (1,)), ((), ()))
                partial[block, :, picked] = (
                    lax.dot_general(
                        grad_gate, gate_mat[picked, :], over_width, preferred_element_type=f32
                    )
                    + lax.dot_general(
                        grad_up, up_mat[picked, :], over_width, preferred_element_type=f32
                    )
                ).astype(bf16)
                return carry

            lax.fori_loop(0, lanes, back, 0)
            to_core(block, 1).start()
            to_core(block, 0).start()

        each_block(level, lambda *at: chosen_now(*at, compute))

    def middle_level(level, chosen_now):
        def middle(block, side, line):
            to_core(block, 1).wait_recv()
            to_far[block] = (
                partial[block, :, columns(far_peer, quarter)].astype(f32)
                + from_core[block, 1].astype(f32)
            ).astype(bf16)
            to_far_peer(block).start()

        each_block(level, lambda *at: chosen_now(*at, middle))

    def total_level(level):
        def total(block, side, line):
            to_core(block, 0).wait_recv()
            to_far_peer(block).wait_recv()
            value = (
                partial[block, :, columns(lane, quarter)].astype(f32)
                + from_core[block, 0].astype(f32)
                + from_far[block].astype(f32)
            ).astype(bf16)

            @pl.when(block == spot)
            def _():
                returned[spot] = value

            @pl.when(block != spot)
            def _():
                from_far[block] = value
                home(block).start()

        each_block(level, total)

    slots = groups * span
    down_in = (((0,), (0,)), ((), ()))
    grad_copies = [
        pltpu.make_async_copy(grad_b, down_out, local_sem.at[0]),
        pltpu.make_async_copy(grad_a.at[0], gate_out, local_sem.at[1]),
        pltpu.make_async_copy(grad_a.at[1], up_out, local_sem.at[2]),
    ]

    def down_grad():

        def down_step(at, carry):
            picked = columns(at, quarter)
            grad_b[:, picked] = lax.dot_general(
                hidden[...].reshape(slots, hidden.shape[2]),
                row_cots[:, :, picked].reshape(slots, quarter),
                down_in,
                preferred_element_type=f32,
            )
            return carry

        lax.fori_loop(0, lanes, down_step, 0)
        grad_copies[0].start()

    def wide_grad(spread, index):
        def step(at, carry):
            picked = columns(at, quarter)
            grad_a[index, picked, :] = lax.dot_general(
                rows[:, :, picked].reshape(slots, quarter),
                spread[...].reshape(slots, spread.shape[2]),
                down_in,
                preferred_element_type=f32,
            )
            return carry

        lax.fori_loop(0, lanes, step, 0)
        grad_copies[index + 1].start()

    def advance(level, carry):
        @pl.when(level == 1)
        def _():
            def hear_all(offset, carry):
                told(offset).wait_recv()
                return carry

            lax.fori_loop(1, groups, hear_all, 0)

        take_narrow(level, 1)
        take_narrow(level, 0)
        take_wide(level, 1)
        share_level(level - 1)
        move_early(level, 0)
        work_level(level - 1, False)
        take_wide(level, 0)
        move_early(level + 1, 1)
        work_level(level, True)
        receive_level(level, 1)

        @pl.when(level < depth)
        def _():
            total_level(level - 1)

        receive_level(level, 0)
        return carry

    lax.fori_loop(0, depth + 1, advance, 0)
    down_grad()
    total_level(depth - 1)
    wide_grad(dgate, 0)
    wide_grad(dup, 1)
    combined[...] = jnp.zeros_like(combined)

    def combine_level(level, carry):
        def combine(block, side, line):
            @pl.when(block != spot)
            def _():
                home_from(block).wait_recv()

            slot = lax.broadcasted_iota(jnp.int32, (token_count, span), 1) + block * span
            slot = slot.astype(f32)
            hit = jnp.logical_or(slot == targets[:, 0:1], slot == targets[:, 1:2])
            picked = jnp.where(hit, 1.0, 0.0).astype(bf16)
            combined[...] += jnp.dot(picked, returned[block], preferred_element_type=f32)

        each_block(level, combine)
        return carry

    lax.fori_loop(-1, depth, combine_level, 0)

    def gather_part(who):
        return gathered.at[:, columns(who, quarter)]

    def gather_copy(index, who, peer):
        held = gather_part(who)
        return remote(held, held, send_g.at[index], recv_g.at[index], tp=peer)

    gathered[:, columns(lane, quarter)] = combined[...].astype(bf16)
    gather_copy(0, lane, far_peer).start()
    gather_copy(1, lane, core_peer).start()
    product[...] = jnp.zeros_like(product)

    def add_product(who):
        wide = columns(who, quarter)

        def step(at, carry):
            picked = pl.ds(pl.multiple_of(at * tall, tall), tall)
            pulled = gathered[picked, wide].astype(f32) * gain[:, wide]
            product[picked, :] += jnp.sum(
                pulled * resid[picked, wide].astype(f32), axis=1, keepdims=True
            )
            return carry

        lax.fori_loop(0, token_count // tall, step, 0)

    add_product(lane)
    gather_copy(1, lane, core_peer).wait_recv()
    add_product(core_peer)
    gather_copy(0, lane, far_peer).wait_recv()
    gather_copy(2, far_peer, core_peer).start()
    add_product(far_peer)
    gather_copy(2, far_peer, core_peer).wait_recv()
    add_product(lax.rem(core_peer + lanes // 2, lanes))

    def resid_strip(at, carry):
        picked = pl.ds(pl.multiple_of(at * strip, strip), strip)
        scale = inverse[picked, :]
        pulled = gathered[picked, :].astype(f32) * gain[...]
        shift_back = scale * scale * scale * (product[picked, :] * (1.0 / model_width))
        resid_grad[picked, :] = (
            cots[picked, :].astype(f32)
            + scale * pulled
            - resid[picked, :].astype(f32) * shift_back
        ).astype(bf16)
        return carry

    lax.fori_loop(0, token_count // strip, resid_strip, 0, unroll=2)
    gather_copy(0, lane, far_peer).wait_send()
    gather_copy(1, lane, core_peer).wait_send()
    gather_copy(2, far_peer, core_peer).wait_send()

    @pl.when(spot < groups - 1)
    def _():
        shift().wait_send()

    @pl.when(spot > 0)
    def _():
        shift().wait_recv()

    for copy in grad_copies:
        copy.wait()

    def finish_info(offset, carry):
        tell(offset).wait_send()
        origin = lax.rem(spot + offset, groups)
        home_from(origin).wait_send()
        return carry

    lax.fori_loop(1, groups, finish_info, 0)
    for k in (0, 1):
        for side in (0, 1):

            @pl.when(onward(side))
            def _():
                by_kind(
                    z,
                    lambda: hop_wide(k, z, side, True).wait_send(),
                    lambda: hop(k, z, side, True).wait_send(),
                )

        over_own(k).wait_send()
        half_copy(k, mate).wait_send()

    def finish_level(level, carry):
        def finish(block, side, line):
            to_core(block, 0).wait_send()
            to_core(block, 1).wait_send()
            to_far_peer(block).wait_send()

            @pl.when(level > 0)
            def _():
                at = source(side, level)

                def done(hold, cross):
                    @pl.when(line == 0)
                    def _():
                        for k in (0, 1):
                            cross(k, at).wait_send()

                            @pl.when(onward(side))
                            def _():
                                hold(k, at, side, False).wait_send()

                def wide():
                    for k in (0, 1):
                        half_copy(k, block).wait_send()
                    done(hop_wide, over_wide)

                def narrow():
                    for k in (0, 1):
                        far_copy(k, block).wait_send()
                        core_copy(k, block).wait_send()
                        pass_copy(k, block).wait_send()
                    done(hop, over)

                by_kind(at, wide, narrow)

        each_block(level, finish)
        return carry

    lax.fori_loop(-1, depth, finish_level, 0)


def experts(
    resid, cots, gain, edge, info, targets, gate_mat, up_mat, down_mat, groups, lanes, span
):
    token_count, model_width = resid.shape
    inner = gate_mat.shape[1]
    quarter = model_width // lanes
    width = 2
    depth = groups // width
    bf16, f32 = jnp.bfloat16, jnp.float32
    dma = pltpu.SemaphoreType.DMA
    inside = pl.BlockSpec(memory_space=pltpu.VMEM)
    anywhere = pl.BlockSpec(memory_space=pl.ANY)
    block = (groups, span, quarter)
    whole = (groups, span, model_width)
    thin = (groups, span, inner)
    vmem = pltpu.VMEM
    return pl.pallas_call(
        functools.partial(expert_kernel, groups, width, lanes),
        out_shape=(
            jax.ShapeDtypeStruct(resid.shape, bf16),
            jax.ShapeDtypeStruct(edge.shape, f32),
            jax.ShapeDtypeStruct(gate_mat.shape, f32),
            jax.ShapeDtypeStruct(up_mat.shape, f32),
            jax.ShapeDtypeStruct(down_mat.shape, f32),
        ),
        in_specs=[inside] * 9,
        out_specs=(inside, inside, anywhere, anywhere, anywhere),
        scratch_shapes=[
            vmem(resid.shape, bf16),
            vmem((token_count, 1), f32),
            vmem((token_count, 1), f32),
            vmem(resid.shape, bf16),
            vmem((groups,) + info.shape, f32),
            vmem((2, depth, token_count, quarter), bf16),
            vmem((2, 2, token_count, model_width // 2), bf16),
            vmem((2, depth, span, quarter), bf16),
            vmem((2, 2, span, model_width // 2), bf16),
            vmem((2, span, model_width // 2), bf16),
            vmem(whole, bf16),
            vmem(whole, bf16),
            vmem(thin, bf16),
            vmem(thin, bf16),
            vmem(thin, bf16),
            vmem(whole, bf16),
            vmem((groups, 2, span, quarter), bf16),
            vmem(block, bf16),
            vmem(block, bf16),
            vmem(block, bf16),
            vmem((token_count, quarter), f32),
            vmem((2,) + gate_mat.shape, f32),
            vmem(down_mat.shape, f32),
            dma((3,)),
            dma((groups,)),
            dma((groups,)),
            dma((2, 2, depth)),
            dma((2, depth)),
            dma((2, depth)),
            dma((2, depth)),
            dma((2,)),
            dma((2,)),
        ]
        + [dma((2, groups))] * 6
        + [dma((groups, 2))] * 2
        + [dma((groups,))] * 4
        + [dma((3,))] * 2
        + [dma((1,))] * 2,
        compiler_params=pltpu.CompilerParams(
            collective_id=1, has_side_effects=True, vmem_limit_bytes=67043328
        ),
        cost_estimate=pl.CostEstimate(
            flops=16 * groups * span * model_width * inner,
            bytes_accessed=150 * 2**20,
            transcendentals=0,
        ),
        name="experts",
    )(resid, cots, gain, edge, info, targets, gate_mat, up_mat, down_mat)


def reduce_kernel(
    groups,
    width,
    lanes,
    partial,
    edge,
    total,
    edge_got,
    from_mate,
    sums,
    arrived,
    send_y,
    recv_y,
    send_z,
    recv_z,
    send_e,
    recv_e,
):
    f32 = jnp.float32
    spot, lane = lax.axis_index("sp"), lax.axis_index("tp")
    depth = groups // width
    z, y = lax.div(spot, width), lax.rem(spot, width)
    mate = spot + 1 - 2 * y
    core_peer = lane + 1 - 2 * lax.rem(lane, 2)
    far_peer = lax.rem(lane + lanes // 2, lanes)

    def goal_of(step):
        return lax.rem(z + step + 1, depth)

    def over(at):
        return remote(
            partial.at[at * width + 1 - y],
            from_mate.at[at],
            send_y.at[at],
            recv_y.at[at],
            sp=mate,
        )

    def along(at):
        return remote(
            sums.at[at], arrived.at[z], send_z.at[at], recv_z.at[z], sp=at * width + y
        )

    def along_from(at):
        return remote(
            sums.at[at], arrived.at[at], send_z.at[at], recv_z.at[at], sp=at * width + y
        )

    def shift():
        goal = lax.rem(spot + groups - 1, groups)
        return remote(edge, edge_got, send_e.at[0], recv_e.at[0], sp=goal)

    greet(groups, spot, core_peer, far_peer)

    @pl.when(spot > 0)
    def _():
        shift().start()

    @pl.when(spot == groups - 1)
    def _():
        edge_got[...] = jnp.zeros_like(edge_got)

    def launch(step, carry):
        over(goal_of(step)).start()
        return carry

    lax.fori_loop(0, depth, launch, 0)

    def pair(step, carry):
        at = goal_of(step)
        over(at).wait_recv()
        both = partial[at * width + y].astype(f32) + from_mate[at].astype(f32)

        @pl.when(at == z)
        def _():
            total[...] = both

        @pl.when(at != z)
        def _():
            sums[at] = both.astype(sums.dtype)
            along(at).start()

        return carry

    lax.fori_loop(0, depth, pair, 0)

    def add(step, carry):
        at = lax.rem(z + depth - 1 - step, depth)
        along_from(at).wait_recv()
        total[...] += arrived[at].astype(f32)
        return carry

    lax.fori_loop(0, depth - 1, add, 0)

    def finish(step, carry):
        at = goal_of(step)
        over(at).wait_send()

        @pl.when(at != z)
        def _():
            along(at).wait_send()

        return carry

    lax.fori_loop(0, depth, finish, 0)

    @pl.when(spot > 0)
    def _():
        shift().wait_send()

    @pl.when(spot < groups - 1)
    def _():
        shift().wait_recv()


def reduce_rows(partial, edge, groups, lanes):
    width = 2
    depth = groups // width
    dma = pltpu.SemaphoreType.DMA
    inside = pl.BlockSpec(memory_space=pltpu.VMEM)
    held = pltpu.VMEM((depth,) + partial.shape[1:], partial.dtype)
    return pl.pallas_call(
        functools.partial(reduce_kernel, groups, width, lanes),
        out_shape=(
            jax.ShapeDtypeStruct(partial.shape[1:], jnp.float32),
            jax.ShapeDtypeStruct(edge.shape, edge.dtype),
        ),
        in_specs=[inside] * 2,
        out_specs=(inside, inside),
        scratch_shapes=[held] * 3 + [dma((depth,))] * 4 + [dma((1,))] * 2,
        compiler_params=pltpu.CompilerParams(collective_id=4, has_side_effects=True),
        name="reduce_rows",
    )(partial, edge)


def hand_kernel(count, parts, *refs):
    given, out, held = refs[:count], refs[count : 2 * count], refs[2 * count : 3 * count]
    come, go = refs[3 * count :]

    def piece(ref, at):
        step = ref.shape[0] // parts
        return ref.at[at * step : (at + 1) * step]

    def inward(k, at):
        return pltpu.make_async_copy(piece(given[k], at), piece(held[k], at), come.at[k, at])

    def outward(k, at):
        return pltpu.make_async_copy(piece(held[k], at), piece(out[k], at), go.at[k, at])

    every = [(k, at) for k in range(count) for at in range(parts)]
    for k, at in every:
        inward(k, at).start()
    for k, at in every:
        inward(k, at).wait()
        outward(k, at).start()
    for k, at in every:
        outward(k, at).wait()


def hand_over(*arrays):
    parts = 2
    count = len(arrays)
    anywhere = pl.BlockSpec(memory_space=pl.ANY)
    dma = pltpu.SemaphoreType.DMA((count, parts))
    return pl.pallas_call(
        functools.partial(hand_kernel, count, parts),
        out_shape=tuple(jax.ShapeDtypeStruct(a.shape, a.dtype) for a in arrays),
        in_specs=[anywhere] * count,
        out_specs=(anywhere,) * count,
        scratch_shapes=[pltpu.VMEM(a.shape, a.dtype) for a in arrays] + [dma, dma],
        name="hand_over",
    )(*arrays)


def on_device(
    resid_in,
    cotangent,
    norm_gain,
    routes,
    route_weights,
    gate_weight,
    up_weight,
    down_weight,
    out_weight,
    gate_b,
    gate_c,
    values_u,
    taps,
):
    f32 = jnp.float32
    bf16 = jnp.bfloat16
    token_count, model_width = resid_in.shape
    groups = lax.axis_size("sp")
    lanes = lax.axis_size("tp")
    local_experts = gate_weight.shape[0]
    expert_total = local_experts * groups
    capacity = 4 * token_count // expert_total
    slot_span = local_experts * capacity
    names = jnp.arange(expert_total, dtype=jnp.int32)
    chosen = routes[:, :, None] == names[None, None, :]
    named = jnp.any(chosen, axis=1).astype(bf16)
    order = jnp.arange(token_count, dtype=jnp.int32)
    strict = (order[:, None] > order[None, :]).astype(bf16)
    before = jnp.dot(strict, named, preferred_element_type=f32).astype(jnp.int32)
    rank = jnp.sum(jnp.where(chosen, before[:, None, :], 0), axis=2)
    targets = routes * capacity + rank
    info = jnp.concatenate(
        [
            targets.T.astype(f32),
            route_weights.T,
            jnp.zeros((4, token_count), f32),
        ],
        axis=0,
    )
    edge = gate_c[-8:].astype(f32) * values_u[-8:].astype(f32)
    grad_resid, earlier, grad_gate, grad_up, grad_down = experts(
        resid_in,
        cotangent,
        norm_gain[None, :],
        edge,
        info,
        targets.astype(f32),
        gate_weight[0],
        up_weight[0],
        down_weight[0],
        groups,
        lanes,
        slot_span,
    )
    mixed = gate_c.astype(f32) * values_u.astype(f32)
    extended = jnp.concatenate([earlier[-2:], mixed], axis=0)
    conv = (
        taps[0] * extended[:token_count]
        + taps[1] * extended[1 : token_count + 1]
        + taps[2] * extended[2 : token_count + 2]
    )
    merged = (gate_b.astype(f32) * conv).astype(bf16)
    out_partial = jnp.einsum("td,tc->dc", grad_resid, merged, preferred_element_type=f32)
    dmerged = jnp.dot(grad_resid, out_weight, preferred_element_type=f32)
    grad_gate_b = (dmerged * conv).astype(bf16)
    dconv = dmerged * gate_b.astype(f32)
    grad_out_weight, later = reduce_rows(
        out_partial.astype(bf16).reshape(groups, model_width // groups, merged.shape[1]),
        dconv[:8],
        groups,
        lanes,
    )
    extended_grad = jnp.concatenate([dconv, later[:2]], axis=0)
    dmixed = (
        taps[2] * extended_grad[:token_count]
        + taps[1] * extended_grad[1 : token_count + 1]
        + taps[0] * extended_grad[2 : token_count + 2]
    )
    grad_gate_c = (dmixed * values_u.astype(f32)).astype(bf16)
    grad_values = (dmixed * gate_c.astype(f32)).astype(bf16)
    grad_gate, grad_up, grad_down, grad_resid_out, grad_out_weight = hand_over(
        grad_gate, grad_up, grad_down, grad_resid, grad_out_weight
    )
    return (
        grad_gate[None],
        grad_up[None],
        grad_down[None],
        grad_resid_out,
        grad_out_weight,
        grad_gate_b,
        grad_gate_c,
        grad_values,
    )


def solution(mesh):
    placed = (
        P("sp", None),
        P("sp", None),
        P(),
        P("sp", None),
        P("sp", None),
        P("sp", None, "tp"),
        P("sp", None, "tp"),
        P("sp", "tp", None),
        P(None, "tp"),
        P("sp", "tp"),
        P("sp", "tp"),
        P("sp", "tp"),
        P(None, "tp"),
    )
    return jax.shard_map(
        on_device,
        mesh=mesh,
        in_specs=placed,
        out_specs=(
            P("sp", None, "tp"),
            P("sp", None, "tp"),
            P("sp", "tp", None),
            P("sp", None),
            P("sp", "tp"),
            P("sp", "tp"),
            P("sp", "tp"),
            P("sp", "tp"),
        ),
        check_vma=False,
    )
```

```python
import functools

import jax
import jax.numpy as jnp
from jax import lax
from jax.experimental import pallas as pl
from jax.experimental.pallas import tpu as pltpu
from jax.sharding import PartitionSpec as P

norm_eps = 1e-06


def remote(source, target, send_sem, recv_sem, **device):
    return pltpu.make_async_remote_copy(
        src_ref=source,
        dst_ref=target,
        send_sem=send_sem,
        recv_sem=recv_sem,
        device_id=device,
        device_id_type=pl.DeviceIdType.MESH,
    )


def greet(groups, spot, core_peer, far_peer):
    barrier = pltpu.get_barrier_semaphore()

    def to_group(offset, carry):
        pl.semaphore_signal(
            barrier,
            inc=1,
            device_id={"sp": lax.rem(spot + offset, groups)},
            device_id_type=pl.DeviceIdType.MESH,
        )
        return carry

    lax.fori_loop(1, groups, to_group, 0)
    for peer in (core_peer, far_peer):
        pl.semaphore_signal(
            barrier, inc=1, device_id={"tp": peer}, device_id_type=pl.DeviceIdType.MESH
        )
    return lambda: pl.semaphore_wait(barrier, groups + 1)


def expert_kernel(
    groups,
    width,
    lanes,
    resid,
    cots,
    gain,
    gate_c,
    values_u,
    routes,
    route_weights,
    gate_mat,
    up_mat,
    down_mat,
    resid_grad,
    edge_got,
    gate_out,
    up_out,
    down_out,
    normed,
    inverse,
    product,
    gathered,
    edge,
    infos,
    dense,
    dense_wide,
    to_mate,
    to_mate_wide,
    to_mate_own,
    rows,
    row_cots,
    hidden,
    dgate,
    dup,
    partial,
    from_core,
    to_far,
    from_far,
    returned,
    combined,
    grad_a,
    grad_b,
    local_sem,
    send_i,
    recv_i,
    send_z,
    recv_z,
    send_y,
    recv_y,
    send_o,
    recv_o,
    send_x,
    recv_x,
    send_c,
    recv_c,
    send_f,
    recv_f,
    send_t,
    recv_t,
    send_r,
    recv_r,
    send_h,
    recv_h,
    send_g,
    recv_g,
    send_e,
    recv_e,
):
    f32 = jnp.float32
    bf16 = jnp.bfloat16
    spot, lane = lax.axis_index("sp"), lax.axis_index("tp")
    depth = groups // width
    z, y = lax.div(spot, width), lax.rem(spot, width)
    core = lax.rem(lane, 2)
    core_peer = lane + 1 - 2 * core
    far_peer = lax.rem(lane + lanes // 2, lanes)
    mate = spot + 1 - 2 * y
    token_count, model_width = resid.shape
    quarter = model_width // lanes
    half = model_width // 2
    span = rows.shape[1]
    strip = 16
    tall = 64
    given = (normed, cots)
    laid = (rows, row_cots)

    def columns(who, size):
        return pl.ds(pl.multiple_of(who * size, size), size)

    def part(ref, block, who):
        return ref.at[block, :, columns(who, quarter)]

    def source(side, level):
        return z + level * (2 * side - 1)

    def valid(side, level):
        at = source(side, level)
        return jnp.logical_and(level > 0, jnp.logical_and(at >= 0, at < depth))

    def present(side, level, line):
        near = jnp.logical_and(side == 0, line == level + 1)
        return jnp.logical_or(valid(side, level), jnp.logical_and(level <= 0, near))

    def onward(side):
        at = z + 1 - 2 * side
        return jnp.logical_and(at >= 0, at < depth)

    def block_of(side, level, line):
        at = source(side, lax.max(level, 0))
        return at * width + lax.rem(y + line, width)

    def tell(offset):
        goal = lax.rem(spot + offset, groups)
        return remote(infos.at[spot], infos.at[spot], send_i.at[offset], recv_i.at[spot], sp=goal)

    def told(offset):
        origin = lax.rem(spot - offset + groups, groups)
        return remote(infos.at[origin], infos.at[origin], send_i.at[offset], recv_i.at[origin], sp=origin)

    def is_end(at):
        return jnp.logical_or(at == 0, at == depth - 1)

    def end_of(at):
        return lax.min(at, 1)

    def by_kind(at, wide, narrow):
        @pl.when(is_end(at))
        def _():
            wide()

        @pl.when(jnp.logical_not(is_end(at)))
        def _():
            narrow()

    def hop_wide(k, at, side, own):
        held = dense_wide.at[k, end_of(at)]
        return remote(
            given[k].at[:, columns(core, half)] if own else held,
            held,
            send_z.at[k, side, at],
            recv_z.at[k, at],
            sp=spot + width * (1 - 2 * side),
        )

    def over_wide(k, at):
        return remote(
            to_mate_wide.at[k, end_of(at)],
            laid[k].at[at * width + y, :, columns(core, half)],
            send_y.at[k, at],
            recv_y.at[k, at],
            sp=mate,
        )

    def hop(k, at, side, own):
        held = dense.at[k, at]
        return remote(
            given[k].at[:, columns(lane, quarter)] if own else held,
            held,
            send_z.at[k, side, at],
            recv_z.at[k, at],
            sp=spot + width * (1 - 2 * side),
        )

    def over(k, at):
        return remote(
            to_mate.at[k, at],
            part(laid[k], at * width + y, lane),
            send_y.at[k, at],
            recv_y.at[k, at],
            sp=mate,
        )

    def over_own(k):
        return remote(
            to_mate_own.at[k],
            laid[k].at[spot, :, columns(core, half)],
            send_o.at[k],
            recv_o.at[k],
            sp=mate,
        )

    def far_copy(k, block):
        held = part(laid[k], block, lane)
        return remote(held, held, send_x.at[k, block], recv_x.at[k, block], tp=far_peer)

    def core_copy(k, block):
        held = part(laid[k], block, lane)
        return remote(held, held, send_c.at[k, block], recv_c.at[k, block], tp=core_peer)

    def half_copy(k, block):
        held = laid[k].at[block, :, columns(core, half)]
        return remote(held, held, send_c.at[k, block], recv_c.at[k, block], tp=core_peer)

    def pass_copy(k, block):
        held = part(laid[k], block, far_peer)
        return remote(held, held, send_f.at[k, block], recv_f.at[k, block], tp=core_peer)

    def to_core(block, far):
        who = lax.rem(core_peer + far * (lanes // 2), lanes)
        return remote(
            part(partial, block, who),
            from_core.at[block, far],
            send_t.at[block, far],
            recv_t.at[block, far],
            tp=core_peer,
        )

    def to_far_peer(block):
        return remote(
            to_far.at[block],
            from_far.at[block],
            send_r.at[block],
            recv_r.at[block],
            tp=far_peer,
        )

    def home(block):
        return remote(
            from_far.at[block], returned.at[spot], send_h.at[block], recv_h.at[spot], sp=block
        )

    def home_from(block):
        return remote(
            from_far.at[block], returned.at[block], send_h.at[block], recv_h.at[block], sp=block
        )

    def matches(block, expert):
        slot = lax.broadcasted_iota(jnp.int32, (span, token_count), 0) + expert * span
        slot = slot.astype(f32)
        return slot == infos[block, 0:1, :], slot == infos[block, 1:2, :]

    def chosen(block, expert):
        first, second = matches(block, expert)
        return jnp.where(jnp.logical_or(first, second), 1.0, 0.0).astype(bf16)

    def weights_of(block):
        first, second = matches(block, spot)
        return jnp.sum(
            jnp.where(first, infos[block, 2:3, :], 0.0)
            + jnp.where(second, infos[block, 3:4, :], 0.0),
            axis=1,
            keepdims=True,
        )

    def placed(matrix, values):
        return jnp.dot(matrix, values, preferred_element_type=f32).astype(bf16)

    def both(body):
        def step(side, carry):
            body(side)
            return carry

        lax.fori_loop(0, 2, step, 0)

    def each_block(level, body):
        def step(at, carry):
            side, line = lax.div(at, 2), lax.rem(at, 2)

            @pl.when(present(side, level, line))
            def _():
                body(block_of(side, level, line), side, line)

            return carry

        lax.fori_loop(0, 4, step, 0)

    all_here = greet(groups, spot, core_peer, far_peer)
    last = edge.shape[0]
    edge[...] = gate_c[token_count - last :, :].astype(f32) * values_u[
        token_count - last :, :
    ].astype(f32)
    named = lax.broadcasted_iota(jnp.int32, (groups, token_count), 0)
    picks = [named == routes[at : at + 1, :] for at in (0, 1)]
    counted = jnp.where(jnp.logical_or(picks[0], picks[1]), 1.0, 0.0).astype(bf16)
    square = (token_count, token_count)
    strict = jnp.where(
        lax.broadcasted_iota(jnp.int32, square, 0) < lax.broadcasted_iota(jnp.int32, square, 1),
        1.0,
        0.0,
    ).astype(bf16)
    before = jnp.dot(counted, strict, preferred_element_type=f32)
    for at in (0, 1):
        rank = jnp.sum(jnp.where(picks[at], before, 0.0), axis=0, keepdims=True)
        first_slot = (routes[at : at + 1, :] * span).astype(f32)
        infos[spot, at : at + 1, :] = first_slot + rank
        infos[spot, at + 2 : at + 3, :] = route_weights[at : at + 1, :]
    all_here()

    def tell_all(offset, carry):
        tell(offset).start()
        return carry

    lax.fori_loop(1, groups, tell_all, 0)
    def shift():
        return remote(
            edge, edge_got, send_e.at[0], recv_e.at[0], sp=lax.rem(spot + 1, groups)
        )

    @pl.when(spot < groups - 1)
    def _():
        shift().start()

    @pl.when(spot == 0)
    def _():
        edge_got[...] = jnp.zeros_like(edge_got)

    def send_own(k):
        for side in (0, 1):

            @pl.when(onward(side))
            def _():
                by_kind(
                    z,
                    lambda: hop_wide(k, z, side, True).start(),
                    lambda: hop(k, z, side, True).start(),
                )

    send_own(1)

    def norm_strip(at, carry):
        picked = pl.ds(pl.multiple_of(at * strip, strip), strip)
        wide = resid[picked, :].astype(f32)
        mean = jnp.sum(wide * wide, axis=1, keepdims=True) * (1.0 / model_width)
        scale = lax.rsqrt(mean + norm_eps)
        inverse[picked, :] = scale
        normed[picked, :] = (wide * scale * gain[...]).astype(bf16)
        return carry

    lax.fori_loop(0, token_count // strip, norm_strip, 0, unroll=2)
    send_own(0)
    mine_there = chosen(spot, mate)
    for k in (1, 0):
        to_mate_own[k] = placed(mine_there, given[k][:, columns(core, half)])
        over_own(k).start()
    mine_here = chosen(spot, spot)

    def lay_own(at, carry):
        for k in (0, 1):
            laid[k][spot, :, columns(at, quarter)] = placed(
                mine_here, given[k][:, columns(at, quarter)]
            )
        return carry

    lax.fori_loop(0, lanes, lay_own, 0)

    def move(copy, k, at, side):
        copy(k, at, side, False).wait_recv()

        @pl.when(onward(side))
        def _():
            copy(k, at, side, False).start()

    def at_ends(level, ends, body):
        def step(side):
            at = source(side, level)
            kind = is_end(at) if ends else jnp.logical_not(is_end(at))

            @pl.when(jnp.logical_and(valid(side, level), kind))
            def _():
                body(side, at, at * width + y)

        both(step)

    def early(side, level):
        return jnp.logical_and(onward(side), level >= 2)

    def take_narrow(level, k):
        def body(side, at, block):
            move(hop, k, at, side)
            values = dense[k, at]
            laid[k][block, :, columns(lane, quarter)] = placed(chosen(block, spot), values)
            far_copy(k, block).start()
            core_copy(k, block).start()
            to_mate[k, at] = placed(chosen(block, mate), values)
            over(k, at).start()

        at_ends(level, False, body)

    def move_early(level, k):
        def body(side, at, block):
            @pl.when(early(side, level))
            def _():
                move(hop_wide, k, at, side)

        at_ends(level, True, body)

    def take_wide(level, k):
        def body(side, at, block):
            @pl.when(jnp.logical_not(early(side, level)))
            def _():
                move(hop_wide, k, at, side)

            end = end_of(at)
            values = dense_wide[k, end]
            to_mate_wide[k, end] = placed(chosen(block, mate), values)
            over_wide(k, at).start()
            laid[k][block, :, columns(core, half)] = placed(chosen(block, spot), values)
            half_copy(k, block).start()

        at_ends(level, True, body)

    def receive_level(level, k):
        def receive(side):
            @pl.when(valid(side, level))
            def _():
                at = source(side, level)
                block = at * width + 1 - y

                def wide():
                    over_wide(k, at).wait_recv()
                    half_copy(k, block).start()

                def narrow():
                    over(k, at).wait_recv()
                    far_copy(k, block).start()
                    core_copy(k, block).start()

                by_kind(at, wide, narrow)

        both(receive)

    def share_level(level):
        @pl.when(level == 0)
        def _():
            for k in (0, 1):
                over_own(k).wait_recv()
                half_copy(k, mate).start()

        def share(block, side, line):
            narrow = jnp.logical_not(is_end(source(side, level)))

            @pl.when(jnp.logical_and(level > 0, narrow))
            def _():
                for k in (0, 1):
                    far_copy(k, block).wait_recv()
                    pass_copy(k, block).start()

        each_block(level, share)

    def ahead(level, side, line):
        return jnp.logical_and(
            jnp.logical_and(level > 0, line == 0), is_end(source(side, level))
        )

    def work_level(level, first):
        def chosen_now(block, side, line, body):
            now = ahead(level, side, line)

            @pl.when(now if first else jnp.logical_not(now))
            def _():
                body(block, side, line)

        compute_level(level, chosen_now)
        middle_level(level, chosen_now)

    def compute_level(level, chosen_now):
        def compute(block, side, line):
            @pl.when(level > 0)
            def _():
                def wide():
                    for k in (0, 1):
                        half_copy(k, block).wait_recv()

                def narrow():
                    for k in (0, 1):
                        core_copy(k, block).wait_recv()
                        pass_copy(k, block).wait_recv()

                by_kind(source(side, level), wide, narrow)

            @pl.when(jnp.logical_and(level == 0, line == 1))
            def _():
                for k in (0, 1):
                    half_copy(k, mate).wait_recv()

            weight = weights_of(block)
            entry_rows = rows[block]
            gate_pre = jnp.dot(entry_rows, gate_mat[...], preferred_element_type=f32)
            up_pre = jnp.dot(entry_rows, up_mat[...], preferred_element_type=f32)
            pulled = lax.dot_general(
                row_cots[block],
                down_mat[...],
                (((1,), (1,)), ((), ())),
                preferred_element_type=f32,
            )
            logistic = jax.nn.sigmoid(gate_pre)
            activated = gate_pre * logistic
            hidden[block] = (activated * up_pre * weight).astype(bf16)
            dhidden = pulled * weight
            grad_gate = (
                dhidden * up_pre * logistic * (1.0 + gate_pre * (1.0 - logistic))
            ).astype(bf16)
            grad_up = (dhidden * activated).astype(bf16)
            dgate[block] = grad_gate
            dup[block] = grad_up

            def back(at, carry):
                picked = columns(at, quarter)
                over_width = (((1,), (1,)), ((), ()))
                partial[block, :, picked] = (
                    lax.dot_general(
                        grad_gate, gate_mat[picked, :], over_width, preferred_element_type=f32
                    )
                    + lax.dot_general(
                        grad_up, up_mat[picked, :], over_width, preferred_element_type=f32
                    )
                ).astype(bf16)
                return carry

            lax.fori_loop(0, lanes, back, 0)
            to_core(block, 1).start()
            to_core(block, 0).start()

        each_block(level, lambda *at: chosen_now(*at, compute))

    def middle_level(level, chosen_now):
        def middle(block, side, line):
            to_core(block, 1).wait_recv()
            to_far[block] = (
                partial[block, :, columns(far_peer, quarter)].astype(f32)
                + from_core[block, 1].astype(f32)
            ).astype(bf16)
            to_far_peer(block).start()

        each_block(level, lambda *at: chosen_now(*at, middle))

    def total_level(level):
        def total(block, side, line):
            to_core(block, 0).wait_recv()
            to_far_peer(block).wait_recv()
            value = (
                partial[block, :, columns(lane, quarter)].astype(f32)
                + from_core[block, 0].astype(f32)
                + from_far[block].astype(f32)
            ).astype(bf16)

            @pl.when(block == spot)
            def _():
                returned[spot] = value

            @pl.when(block != spot)
            def _():
                from_far[block] = value
                home(block).start()

        each_block(level, total)

    slots = groups * span
    down_in = (((0,), (0,)), ((), ()))
    grad_copies = [
        pltpu.make_async_copy(grad_b, down_out, local_sem.at[0]),
        pltpu.make_async_copy(grad_a.at[0], gate_out, local_sem.at[1]),
        pltpu.make_async_copy(grad_a.at[1], up_out, local_sem.at[2]),
    ]

    def down_grad():

        def down_step(at, carry):
            picked = columns(at, quarter)
            grad_b[:, picked] = lax.dot_general(
                hidden[...].reshape(slots, hidden.shape[2]),
                row_cots[:, :, picked].reshape(slots, quarter),
                down_in,
                preferred_element_type=f32,
            )
            return carry

        lax.fori_loop(0, lanes, down_step, 0)
        grad_copies[0].start()

    def wide_grad(spread, index):
        def step(at, carry):
            picked = columns(at, quarter)
            grad_a[index, picked, :] = lax.dot_general(
                rows[:, :, picked].reshape(slots, quarter),
                spread[...].reshape(slots, spread.shape[2]),
                down_in,
                preferred_element_type=f32,
            )
            return carry

        lax.fori_loop(0, lanes, step, 0)
        grad_copies[index + 1].start()

    def advance(level, carry):
        @pl.when(level == 1)
        def _():
            def hear_all(offset, carry):
                told(offset).wait_recv()
                return carry

            lax.fori_loop(1, groups, hear_all, 0)

        take_narrow(level, 1)
        take_narrow(level, 0)
        take_wide(level, 1)
        share_level(level - 1)
        move_early(level, 0)
        work_level(level - 1, False)
        take_wide(level, 0)
        move_early(level + 1, 1)
        work_level(level, True)
        receive_level(level, 1)

        @pl.when(level < depth)
        def _():
            total_level(level - 1)

        receive_level(level, 0)
        return carry

    lax.fori_loop(0, depth + 1, advance, 0)
    down_grad()
    total_level(depth - 1)
    wide_grad(dgate, 0)
    wide_grad(dup, 1)
    combined[...] = jnp.zeros_like(combined)

    def combine_level(level, carry):
        def combine(block, side, line):
            @pl.when(block != spot)
            def _():
                home_from(block).wait_recv()

            combined[...] += lax.dot_general(
                chosen(spot, block), returned[block], down_in, preferred_element_type=f32
            )

        each_block(level, combine)
        return carry

    lax.fori_loop(-1, depth, combine_level, 0)

    def gather_part(who):
        return gathered.at[:, columns(who, quarter)]

    def gather_copy(index, who, peer):
        held = gather_part(who)
        return remote(held, held, send_g.at[index], recv_g.at[index], tp=peer)

    gathered[:, columns(lane, quarter)] = combined[...].astype(bf16)
    gather_copy(0, lane, far_peer).start()
    gather_copy(1, lane, core_peer).start()
    product[...] = jnp.zeros_like(product)

    def add_product(who):
        wide = columns(who, quarter)

        def step(at, carry):
            picked = pl.ds(pl.multiple_of(at * tall, tall), tall)
            pulled = gathered[picked, wide].astype(f32) * gain[:, wide]
            product[picked, :] += jnp.sum(
                pulled * resid[picked, wide].astype(f32), axis=1, keepdims=True
            )
            return carry

        lax.fori_loop(0, token_count // tall, step, 0)

    add_product(lane)
    gather_copy(1, lane, core_peer).wait_recv()
    add_product(core_peer)
    gather_copy(0, lane, far_peer).wait_recv()
    gather_copy(2, far_peer, core_peer).start()
    add_product(far_peer)
    gather_copy(2, far_peer, core_peer).wait_recv()
    add_product(lax.rem(core_peer + lanes // 2, lanes))

    def resid_strip(at, carry):
        picked = pl.ds(pl.multiple_of(at * strip, strip), strip)
        scale = inverse[picked, :]
        pulled = gathered[picked, :].astype(f32) * gain[...]
        shift_back = scale * scale * scale * (product[picked, :] * (1.0 / model_width))
        resid_grad[picked, :] = (
            cots[picked, :].astype(f32)
            + scale * pulled
            - resid[picked, :].astype(f32) * shift_back
        ).astype(bf16)
        return carry

    lax.fori_loop(0, token_count // strip, resid_strip, 0, unroll=2)
    gather_copy(0, lane, far_peer).wait_send()
    gather_copy(1, lane, core_peer).wait_send()
    gather_copy(2, far_peer, core_peer).wait_send()

    @pl.when(spot < groups - 1)
    def _():
        shift().wait_send()

    @pl.when(spot > 0)
    def _():
        shift().wait_recv()

    for copy in grad_copies:
        copy.wait()

    def finish_info(offset, carry):
        tell(offset).wait_send()
        origin = lax.rem(spot + offset, groups)
        home_from(origin).wait_send()
        return carry

    lax.fori_loop(1, groups, finish_info, 0)
    for k in (0, 1):
        for side in (0, 1):

            @pl.when(onward(side))
            def _():
                by_kind(
                    z,
                    lambda: hop_wide(k, z, side, True).wait_send(),
                    lambda: hop(k, z, side, True).wait_send(),
                )

        over_own(k).wait_send()
        half_copy(k, mate).wait_send()

    def finish_level(level, carry):
        def finish(block, side, line):
            to_core(block, 0).wait_send()
            to_core(block, 1).wait_send()
            to_far_peer(block).wait_send()

            @pl.when(level > 0)
            def _():
                at = source(side, level)

                def done(hold, cross):
                    @pl.when(line == 0)
                    def _():
                        for k in (0, 1):
                            cross(k, at).wait_send()

                            @pl.when(onward(side))
                            def _():
                                hold(k, at, side, False).wait_send()

                def wide():
                    for k in (0, 1):
                        half_copy(k, block).wait_send()
                    done(hop_wide, over_wide)

                def narrow():
                    for k in (0, 1):
                        far_copy(k, block).wait_send()
                        core_copy(k, block).wait_send()
                        pass_copy(k, block).wait_send()
                    done(hop, over)

                by_kind(at, wide, narrow)

        each_block(level, finish)
        return carry

    lax.fori_loop(-1, depth, finish_level, 0)


def experts(
    resid,
    cots,
    gain,
    gate_c,
    values_u,
    routes,
    route_weights,
    gate_mat,
    up_mat,
    down_mat,
    groups,
    lanes,
    span,
):
    token_count, model_width = resid.shape
    inner = gate_mat.shape[1]
    quarter = model_width // lanes
    width = 2
    depth = groups // width
    bf16, f32 = jnp.bfloat16, jnp.float32
    dma = pltpu.SemaphoreType.DMA
    inside = pl.BlockSpec(memory_space=pltpu.VMEM)
    anywhere = pl.BlockSpec(memory_space=pl.ANY)
    block = (groups, span, quarter)
    whole = (groups, span, model_width)
    thin = (groups, span, inner)
    edge_shape = (16, gate_c.shape[1])
    vmem = pltpu.VMEM
    return pl.pallas_call(
        functools.partial(expert_kernel, groups, width, lanes),
        out_shape=(
            jax.ShapeDtypeStruct(resid.shape, bf16),
            jax.ShapeDtypeStruct(edge_shape, f32),
            jax.ShapeDtypeStruct(gate_mat.shape, f32),
            jax.ShapeDtypeStruct(up_mat.shape, f32),
            jax.ShapeDtypeStruct(down_mat.shape, f32),
        ),
        in_specs=[inside] * 10,
        out_specs=(inside, inside, anywhere, anywhere, anywhere),
        scratch_shapes=[
            vmem(resid.shape, bf16),
            vmem((token_count, 1), f32),
            vmem((token_count, 1), f32),
            vmem(resid.shape, bf16),
            vmem(edge_shape, f32),
            vmem((groups, 8, token_count), f32),
            vmem((2, depth, token_count, quarter), bf16),
            vmem((2, 2, token_count, model_width // 2), bf16),
            vmem((2, depth, span, quarter), bf16),
            vmem((2, 2, span, model_width // 2), bf16),
            vmem((2, span, model_width // 2), bf16),
            vmem(whole, bf16),
            vmem(whole, bf16),
            vmem(thin, bf16),
            vmem(thin, bf16),
            vmem(thin, bf16),
            vmem(whole, bf16),
            vmem((groups, 2, span, quarter), bf16),
            vmem(block, bf16),
            vmem(block, bf16),
            vmem(block, bf16),
            vmem((token_count, quarter), f32),
            vmem((2,) + gate_mat.shape, f32),
            vmem(down_mat.shape, f32),
            dma((3,)),
            dma((groups,)),
            dma((groups,)),
            dma((2, 2, depth)),
            dma((2, depth)),
            dma((2, depth)),
            dma((2, depth)),
            dma((2,)),
            dma((2,)),
        ]
        + [dma((2, groups))] * 6
        + [dma((groups, 2))] * 2
        + [dma((groups,))] * 4
        + [dma((3,))] * 2
        + [dma((1,))] * 2,
        compiler_params=pltpu.CompilerParams(
            collective_id=1, has_side_effects=True, vmem_limit_bytes=67043328
        ),
        cost_estimate=pl.CostEstimate(
            flops=16 * groups * span * model_width * inner,
            bytes_accessed=150 * 2**20,
            transcendentals=0,
        ),
        name="experts",
    )(
        resid,
        cots,
        gain,
        gate_c,
        values_u,
        routes,
        route_weights,
        gate_mat,
        up_mat,
        down_mat,
    )


def tail_kernel(
    groups,
    width,
    lanes,
    pieces,
    resid_grad,
    earlier,
    out_mat,
    gate_b,
    gate_c,
    values_u,
    taps,
    total,
    grad_b,
    grad_c,
    grad_u,
    partial,
    mixed,
    conv,
    merged,
    pulled,
    edge,
    edge_got,
    from_mate,
    sums,
    arrived,
    send_y,
    recv_y,
    send_z,
    recv_z,
    send_e,
    recv_e,
):
    f32 = jnp.float32
    bf16 = jnp.bfloat16
    spot, lane = lax.axis_index("sp"), lax.axis_index("tp")
    depth = groups // width
    z, y = lax.div(spot, width), lax.rem(spot, width)
    mate = spot + 1 - 2 * y
    core_peer = lane + 1 - 2 * lax.rem(lane, 2)
    far_peer = lax.rem(lane + lanes // 2, lanes)
    token_count, model_width = resid_grad.shape
    piece = model_width // pieces
    per = depth // pieces
    lead = earlier.shape[0]

    def goal_of(step):
        return lax.rem(z + step + 1, depth)

    def over(at):
        return remote(
            partial.at[at * width + 1 - y],
            from_mate.at[at],
            send_y.at[at],
            recv_y.at[at],
            sp=mate,
        )

    def along(at):
        return remote(
            sums.at[at], arrived.at[z], send_z.at[at], recv_z.at[z], sp=at * width + y
        )

    def along_from(at):
        return remote(
            sums.at[at], arrived.at[at], send_z.at[at], recv_z.at[at], sp=at * width + y
        )

    def shift():
        goal = lax.rem(spot + groups - 1, groups)
        return remote(edge, edge_got, send_e.at[0], recv_e.at[0], sp=goal)

    all_here = greet(groups, spot, core_peer, far_peer)
    mixed[0:lead, :] = earlier[...]
    mixed[lead:, :] = gate_c[...].astype(f32) * values_u[...].astype(f32)
    conv[...] = (
        taps[0:1, :] * mixed[lead - 2 : lead - 2 + token_count, :]
        + taps[1:2, :] * mixed[lead - 1 : lead - 1 + token_count, :]
        + taps[2:3, :] * mixed[lead : lead + token_count, :]
    )
    merged[...] = (gate_b[...].astype(f32) * conv[...]).astype(bf16)

    def make(step):
        at = lax.rem(lax.div(z, per) + step + 1, pieces)
        made = lax.dot_general(
            resid_grad[:, pl.ds(pl.multiple_of(at * piece, piece), piece)],
            merged[...],
            (((0,), (0,)), ((), ())),
            preferred_element_type=f32,
        ).astype(bf16)
        count = per * width
        partial[pl.ds(at * count, count)] = made.reshape((count,) + partial.shape[1:])
        return at

    first = make(0)
    all_here()

    def launch(at):
        def step(k, carry):
            over(at * per + k).start()
            return carry

        lax.fori_loop(0, per, step, 0)

    launch(first)

    def make_next(step, carry):
        launch(make(step))
        return carry

    lax.fori_loop(1, pieces, make_next, 0)
    dmerged = jnp.dot(resid_grad[...], out_mat[...], preferred_element_type=f32)
    pulled[0:token_count, :] = dmerged * gate_b[...].astype(f32)
    edge[...] = pulled[0 : edge.shape[0], :]

    @pl.when(spot > 0)
    def _():
        shift().start()

    @pl.when(spot == groups - 1)
    def _():
        edge_got[...] = jnp.zeros_like(edge_got)

    grad_b[...] = (dmerged * conv[...]).astype(bf16)

    def pair(step, carry):
        at = goal_of(step)
        over(at).wait_recv()
        both = partial[at * width + y].astype(f32) + from_mate[at].astype(f32)

        @pl.when(at == z)
        def _():
            total[...] = both

        @pl.when(at != z)
        def _():
            sums[at] = both.astype(sums.dtype)
            along(at).start()

        return carry

    lax.fori_loop(0, depth, pair, 0)

    @pl.when(spot < groups - 1)
    def _():
        shift().wait_recv()

    pulled[token_count:, :] = edge_got[...]
    dmixed = (
        taps[2:3, :] * pulled[0:token_count, :]
        + taps[1:2, :] * pulled[1 : token_count + 1, :]
        + taps[0:1, :] * pulled[2 : token_count + 2, :]
    )
    grad_c[...] = (dmixed * values_u[...].astype(f32)).astype(bf16)
    grad_u[...] = (dmixed * gate_c[...].astype(f32)).astype(bf16)

    def add(step, carry):
        at = lax.rem(z + depth - 1 - step, depth)
        along_from(at).wait_recv()
        total[...] += arrived[at].astype(f32)
        return carry

    lax.fori_loop(0, depth - 1, add, 0)

    def finish(step, carry):
        at = goal_of(step)
        over(at).wait_send()

        @pl.when(at != z)
        def _():
            along(at).wait_send()

        return carry

    lax.fori_loop(0, depth, finish, 0)

    @pl.when(spot > 0)
    def _():
        shift().wait_send()


def tail(resid_grad, earlier, out_mat, gate_b, gate_c, values_u, taps, groups, lanes):
    width = 2
    depth = groups // width
    pieces = lanes if depth % lanes == 0 else 1
    token_count, model_width = resid_grad.shape
    channels = out_mat.shape[1]
    bf16, f32 = jnp.bfloat16, jnp.float32
    dma = pltpu.SemaphoreType.DMA
    vmem = pltpu.VMEM
    inside = pl.BlockSpec(memory_space=vmem)
    block = (model_width // groups, channels)
    flat = (token_count, channels)
    edge_shape = (8, channels)
    held = vmem((depth,) + block, bf16)
    return pl.pallas_call(
        functools.partial(tail_kernel, groups, width, lanes, pieces),
        out_shape=(jax.ShapeDtypeStruct(block, f32),)
        + (jax.ShapeDtypeStruct(flat, bf16),) * 3,
        in_specs=[inside] * 7,
        out_specs=(inside,) * 4,
        scratch_shapes=[
            vmem((groups,) + block, bf16),
            vmem((token_count + earlier.shape[0], channels), f32),
            vmem(flat, f32),
            vmem(flat, bf16),
            vmem((token_count + 8, channels), f32),
            vmem(edge_shape, f32),
            vmem(edge_shape, f32),
            held,
            held,
            held,
        ]
        + [dma((depth,))] * 4
        + [dma((1,))] * 2,
        compiler_params=pltpu.CompilerParams(
            collective_id=4, has_side_effects=True, vmem_limit_bytes=67043328
        ),
        name="tail",
    )(resid_grad, earlier, out_mat, gate_b, gate_c, values_u, taps)


def hand_kernel(count, parts, *refs):
    given, out, held = refs[:count], refs[count : 2 * count], refs[2 * count : 3 * count]
    come, go = refs[3 * count :]

    def piece(ref, at):
        step = ref.shape[0] // parts
        return ref.at[at * step : (at + 1) * step]

    def inward(k, at):
        return pltpu.make_async_copy(piece(given[k], at), piece(held[k], at), come.at[k, at])

    def outward(k, at):
        return pltpu.make_async_copy(piece(held[k], at), piece(out[k], at), go.at[k, at])

    every = [(k, at) for k in range(count) for at in range(parts)]
    for k, at in every:
        inward(k, at).start()
    for k, at in every:
        inward(k, at).wait()
        outward(k, at).start()
    for k, at in every:
        outward(k, at).wait()


def hand_over(*arrays):
    parts = 2
    count = len(arrays)
    anywhere = pl.BlockSpec(memory_space=pl.ANY)
    dma = pltpu.SemaphoreType.DMA((count, parts))
    return pl.pallas_call(
        functools.partial(hand_kernel, count, parts),
        out_shape=tuple(jax.ShapeDtypeStruct(a.shape, a.dtype) for a in arrays),
        in_specs=[anywhere] * count,
        out_specs=(anywhere,) * count,
        scratch_shapes=[pltpu.VMEM(a.shape, a.dtype) for a in arrays] + [dma, dma],
        compiler_params=pltpu.CompilerParams(vmem_limit_bytes=67043328),
        name="hand_over",
    )(*arrays)


def on_device(
    resid_in,
    cotangent,
    norm_gain,
    routes,
    route_weights,
    gate_weight,
    up_weight,
    down_weight,
    out_weight,
    gate_b,
    gate_c,
    values_u,
    taps,
):
    groups = lax.axis_size("sp")
    lanes = lax.axis_size("tp")
    expert_total = gate_weight.shape[0] * groups
    capacity = 4 * resid_in.shape[0] // expert_total
    grad_resid, earlier, grad_gate, grad_up, grad_down = experts(
        resid_in,
        cotangent,
        norm_gain[None, :],
        gate_c,
        values_u,
        routes.T,
        route_weights.T,
        gate_weight[0],
        up_weight[0],
        down_weight[0],
        groups,
        lanes,
        gate_weight.shape[0] * capacity,
    )
    given = tail(
        grad_resid, earlier, out_weight, gate_b, gate_c, values_u, taps, groups, lanes
    )
    results = hand_over(grad_gate, grad_up, grad_down, grad_resid, *given)
    return tuple(array[None] for array in results[:3]) + tuple(results[3:])


def solution(mesh):
    placed = (
        P("sp", None),
        P("sp", None),
        P(),
        P("sp", None),
        P("sp", None),
        P("sp", None, "tp"),
        P("sp", None, "tp"),
        P("sp", "tp", None),
        P(None, "tp"),
        P("sp", "tp"),
        P("sp", "tp"),
        P("sp", "tp"),
        P(None, "tp"),
    )
    return jax.shard_map(
        on_device,
        mesh=mesh,
        in_specs=placed,
        out_specs=(
            P("sp", None, "tp"),
            P("sp", None, "tp"),
            P("sp", "tp", None),
            P("sp", None),
            P("sp", "tp"),
            P("sp", "tp"),
            P("sp", "tp"),
            P("sp", "tp"),
        ),
        check_vma=False,
    )
```

```python
import functools

import jax
import jax.numpy as jnp
from jax import lax
from jax.experimental import pallas as pl
from jax.experimental.pallas import tpu as pltpu
from jax.sharding import PartitionSpec as P

norm_eps = 1e-06


def remote(source, target, send_sem, recv_sem, **device):
    return pltpu.make_async_remote_copy(
        src_ref=source,
        dst_ref=target,
        send_sem=send_sem,
        recv_sem=recv_sem,
        device_id=device,
        device_id_type=pl.DeviceIdType.MESH,
    )


def greet(groups, spot, core_peer, far_peer):
    barrier = pltpu.get_barrier_semaphore()

    def to_group(offset, carry):
        pl.semaphore_signal(
            barrier,
            inc=1,
            device_id={"sp": lax.rem(spot + offset, groups)},
            device_id_type=pl.DeviceIdType.MESH,
        )
        return carry

    lax.fori_loop(1, groups, to_group, 0)
    for peer in (core_peer, far_peer):
        pl.semaphore_signal(
            barrier, inc=1, device_id={"tp": peer}, device_id_type=pl.DeviceIdType.MESH
        )
    return lambda: pl.semaphore_wait(barrier, groups + 1)


def expert_kernel(
    groups,
    width,
    lanes,
    resid,
    cots,
    gain,
    gate_c,
    values_u,
    routes,
    route_weights,
    gate_mat,
    up_mat,
    down_mat,
    resid_grad,
    edge_got,
    gate_out,
    up_out,
    down_out,
    normed,
    inverse,
    product,
    gathered,
    edge,
    infos,
    dense,
    dense_wide,
    to_mate,
    to_mate_wide,
    to_mate_own,
    rows,
    row_cots,
    hidden,
    dgate,
    dup,
    partial,
    from_core,
    to_far,
    from_far,
    returned,
    combined,
    grad_a,
    grad_b,
    local_sem,
    send_i,
    recv_i,
    send_z,
    recv_z,
    send_y,
    recv_y,
    send_o,
    recv_o,
    send_x,
    recv_x,
    send_c,
    recv_c,
    send_f,
    recv_f,
    send_t,
    recv_t,
    send_r,
    recv_r,
    send_h,
    recv_h,
    send_g,
    recv_g,
    send_e,
    recv_e,
):
    f32 = jnp.float32
    bf16 = jnp.bfloat16
    spot, lane = lax.axis_index("sp"), lax.axis_index("tp")
    depth = groups // width
    z, y = lax.div(spot, width), lax.rem(spot, width)
    core = lax.rem(lane, 2)
    core_peer = lane + 1 - 2 * core
    far_peer = lax.rem(lane + lanes // 2, lanes)
    mate = spot + 1 - 2 * y
    token_count, model_width = resid.shape
    quarter = model_width // lanes
    half = model_width // 2
    span = rows.shape[1]
    strip = 16
    tall = 64
    given = (normed, cots)
    laid = (rows, row_cots)

    def columns(who, size):
        return pl.ds(pl.multiple_of(who * size, size), size)

    def part(ref, block, who):
        return ref.at[block, :, columns(who, quarter)]

    def source(side, level):
        return z + level * (2 * side - 1)

    def valid(side, level):
        at = source(side, level)
        return jnp.logical_and(level > 0, jnp.logical_and(at >= 0, at < depth))

    def present(side, level, line):
        near = jnp.logical_and(side == 0, line == level + 1)
        return jnp.logical_or(valid(side, level), jnp.logical_and(level <= 0, near))

    def onward(side):
        at = z + 1 - 2 * side
        return jnp.logical_and(at >= 0, at < depth)

    def block_of(side, level, line):
        at = source(side, lax.max(level, 0))
        return at * width + lax.rem(y + line, width)

    def tell(offset):
        goal = lax.rem(spot + offset, groups)
        return remote(infos.at[spot], infos.at[spot], send_i.at[offset], recv_i.at[spot], sp=goal)

    def told(offset):
        origin = lax.rem(spot - offset + groups, groups)
        return remote(infos.at[origin], infos.at[origin], send_i.at[offset], recv_i.at[origin], sp=origin)

    def is_end(at):
        return jnp.logical_or(at == 0, at == depth - 1)

    def end_of(at):
        return lax.min(at, 1)

    def by_kind(at, wide, narrow):
        @pl.when(is_end(at))
        def _():
            wide()

        @pl.when(jnp.logical_not(is_end(at)))
        def _():
            narrow()

    def hop_wide(k, at, side, own):
        held = dense_wide.at[k, end_of(at)]
        return remote(
            given[k].at[:, columns(core, half)] if own else held,
            held,
            send_z.at[k, side, at],
            recv_z.at[k, at],
            sp=spot + width * (1 - 2 * side),
        )

    def over_wide(k, at):
        return remote(
            to_mate_wide.at[k, end_of(at)],
            laid[k].at[at * width + y, :, columns(core, half)],
            send_y.at[k, at],
            recv_y.at[k, at],
            sp=mate,
        )

    def hop(k, at, side, own):
        held = dense.at[k, at]
        return remote(
            given[k].at[:, columns(lane, quarter)] if own else held,
            held,
            send_z.at[k, side, at],
            recv_z.at[k, at],
            sp=spot + width * (1 - 2 * side),
        )

    def over(k, at):
        return remote(
            to_mate.at[k, at],
            part(laid[k], at * width + y, lane),
            send_y.at[k, at],
            recv_y.at[k, at],
            sp=mate,
        )

    def over_own(k):
        return remote(
            to_mate_own.at[k],
            laid[k].at[spot, :, columns(core, half)],
            send_o.at[k],
            recv_o.at[k],
            sp=mate,
        )

    def far_copy(k, block):
        held = part(laid[k], block, lane)
        return remote(held, held, send_x.at[k, block], recv_x.at[k, block], tp=far_peer)

    def core_copy(k, block):
        held = part(laid[k], block, lane)
        return remote(held, held, send_c.at[k, block], recv_c.at[k, block], tp=core_peer)

    def half_copy(k, block):
        held = laid[k].at[block, :, columns(core, half)]
        return remote(held, held, send_c.at[k, block], recv_c.at[k, block], tp=core_peer)

    def pass_copy(k, block):
        held = part(laid[k], block, far_peer)
        return remote(held, held, send_f.at[k, block], recv_f.at[k, block], tp=core_peer)

    def to_core(block, far):
        who = lax.rem(core_peer + far * (lanes // 2), lanes)
        return remote(
            part(partial, block, who),
            from_core.at[block, far],
            send_t.at[block, far],
            recv_t.at[block, far],
            tp=core_peer,
        )

    def to_far_peer(block):
        return remote(
            to_far.at[block],
            from_far.at[block],
            send_r.at[block],
            recv_r.at[block],
            tp=far_peer,
        )

    def home(block):
        return remote(
            from_far.at[block], returned.at[spot], send_h.at[block], recv_h.at[spot], sp=block
        )

    def home_from(block):
        return remote(
            from_far.at[block], returned.at[block], send_h.at[block], recv_h.at[block], sp=block
        )

    def matches(block, expert):
        slot = lax.broadcasted_iota(jnp.int32, (span, token_count), 0) + expert * span
        slot = slot.astype(f32)
        return slot == infos[block, 0:1, :], slot == infos[block, 1:2, :]

    def chosen(block, expert):
        first, second = matches(block, expert)
        return jnp.where(jnp.logical_or(first, second), 1.0, 0.0).astype(bf16)

    def weights_of(block):
        first, second = matches(block, spot)
        return jnp.sum(
            jnp.where(first, infos[block, 2:3, :], 0.0)
            + jnp.where(second, infos[block, 3:4, :], 0.0),
            axis=1,
            keepdims=True,
        )

    def placed(matrix, values):
        return jnp.dot(matrix, values, preferred_element_type=f32).astype(bf16)

    def both(body):
        def step(side, carry):
            body(side)
            return carry

        lax.fori_loop(0, 2, step, 0)

    def each_block(level, body):
        def step(at, carry):
            side, line = lax.div(at, 2), lax.rem(at, 2)

            @pl.when(present(side, level, line))
            def _():
                body(block_of(side, level, line), side, line)

            return carry

        lax.fori_loop(0, 4, step, 0)

    all_here = greet(groups, spot, core_peer, far_peer)
    last = edge.shape[0]
    edge[...] = gate_c[token_count - last :, :].astype(f32) * values_u[
        token_count - last :, :
    ].astype(f32)
    named = lax.broadcasted_iota(jnp.int32, (groups, token_count), 0)
    picks = [named == routes[at : at + 1, :] for at in (0, 1)]
    counted = jnp.where(jnp.logical_or(picks[0], picks[1]), 1.0, 0.0).astype(bf16)
    square = (token_count, token_count)
    strict = jnp.where(
        lax.broadcasted_iota(jnp.int32, square, 0) < lax.broadcasted_iota(jnp.int32, square, 1),
        1.0,
        0.0,
    ).astype(bf16)
    before = jnp.dot(counted, strict, preferred_element_type=f32)
    for at in (0, 1):
        rank = jnp.sum(jnp.where(picks[at], before, 0.0), axis=0, keepdims=True)
        first_slot = (routes[at : at + 1, :] * span).astype(f32)
        infos[spot, at : at + 1, :] = first_slot + rank
        infos[spot, at + 2 : at + 3, :] = route_weights[at : at + 1, :]
    all_here()

    def tell_all(offset, carry):
        tell(offset).start()
        return carry

    lax.fori_loop(1, groups, tell_all, 0)
    def shift():
        return remote(
            edge, edge_got, send_e.at[0], recv_e.at[0], sp=lax.rem(spot + 1, groups)
        )

    @pl.when(spot < groups - 1)
    def _():
        shift().start()

    @pl.when(spot == 0)
    def _():
        edge_got[...] = jnp.zeros_like(edge_got)

    def send_own(k):
        for side in (0, 1):

            @pl.when(onward(side))
            def _():
                by_kind(
                    z,
                    lambda: hop_wide(k, z, side, True).start(),
                    lambda: hop(k, z, side, True).start(),
                )

    send_own(1)

    def norm_strip(at, carry):
        picked = pl.ds(pl.multiple_of(at * strip, strip), strip)
        wide = resid[picked, :].astype(f32)
        mean = jnp.sum(wide * wide, axis=1, keepdims=True) * (1.0 / model_width)
        scale = lax.rsqrt(mean + norm_eps)
        inverse[picked, :] = scale
        normed[picked, :] = (wide * scale * gain[...]).astype(bf16)
        return carry

    lax.fori_loop(0, token_count // strip, norm_strip, 0, unroll=2)
    send_own(0)
    mine_there = chosen(spot, mate)
    for k in (1, 0):
        to_mate_own[k] = placed(mine_there, given[k][:, columns(core, half)])
        over_own(k).start()
    mine_here = chosen(spot, spot)

    def lay_own(at, carry):
        for k in (0, 1):
            laid[k][spot, :, columns(at, quarter)] = placed(
                mine_here, given[k][:, columns(at, quarter)]
            )
        return carry

    lax.fori_loop(0, lanes, lay_own, 0)

    def move(copy, k, at, side):
        copy(k, at, side, False).wait_recv()

        @pl.when(onward(side))
        def _():
            copy(k, at, side, False).start()

    def at_ends(level, ends, body):
        def step(side):
            at = source(side, level)
            kind = is_end(at) if ends else jnp.logical_not(is_end(at))

            @pl.when(jnp.logical_and(valid(side, level), kind))
            def _():
                body(side, at, at * width + y)

        both(step)

    def early(side, level):
        return jnp.logical_and(onward(side), level >= 2)

    def take_narrow(level, k):
        def body(side, at, block):
            move(hop, k, at, side)
            values = dense[k, at]
            laid[k][block, :, columns(lane, quarter)] = placed(chosen(block, spot), values)
            far_copy(k, block).start()
            core_copy(k, block).start()
            to_mate[k, at] = placed(chosen(block, mate), values)
            over(k, at).start()

        at_ends(level, False, body)

    def move_early(level, k):
        def body(side, at, block):
            @pl.when(early(side, level))
            def _():
                move(hop_wide, k, at, side)

        at_ends(level, True, body)

    def take_wide(level, k):
        def body(side, at, block):
            @pl.when(jnp.logical_not(early(side, level)))
            def _():
                move(hop_wide, k, at, side)

            end = end_of(at)
            values = dense_wide[k, end]
            to_mate_wide[k, end] = placed(chosen(block, mate), values)
            over_wide(k, at).start()
            laid[k][block, :, columns(core, half)] = placed(chosen(block, spot), values)
            half_copy(k, block).start()

        at_ends(level, True, body)

    def receive_level(level, k):
        def receive(side):
            @pl.when(valid(side, level))
            def _():
                at = source(side, level)
                block = at * width + 1 - y

                def wide():
                    over_wide(k, at).wait_recv()
                    half_copy(k, block).start()

                def narrow():
                    over(k, at).wait_recv()
                    far_copy(k, block).start()
                    core_copy(k, block).start()

                by_kind(at, wide, narrow)

        both(receive)

    def share_level(level):
        @pl.when(level == 0)
        def _():
            for k in (0, 1):
                over_own(k).wait_recv()
                half_copy(k, mate).start()

        def share(block, side, line):
            narrow = jnp.logical_not(is_end(source(side, level)))

            @pl.when(jnp.logical_and(level > 0, narrow))
            def _():
                for k in (0, 1):
                    far_copy(k, block).wait_recv()
                    pass_copy(k, block).start()

        each_block(level, share)

    def ahead(level, side, line):
        return jnp.logical_and(
            jnp.logical_and(level > 0, line == 0), is_end(source(side, level))
        )

    def work_level(level, first):
        def chosen_now(block, side, line, body):
            now = ahead(level, side, line)

            @pl.when(now if first else jnp.logical_not(now))
            def _():
                body(block, side, line)

        compute_level(level, chosen_now)
        middle_level(level, chosen_now)

    def compute_level(level, chosen_now):
        def compute(block, side, line):
            @pl.when(level > 0)
            def _():
                def wide():
                    for k in (0, 1):
                        half_copy(k, block).wait_recv()

                def narrow():
                    for k in (0, 1):
                        core_copy(k, block).wait_recv()
                        pass_copy(k, block).wait_recv()

                by_kind(source(side, level), wide, narrow)

            @pl.when(jnp.logical_and(level == 0, line == 1))
            def _():
                for k in (0, 1):
                    half_copy(k, mate).wait_recv()

            weight = weights_of(block)
            entry_rows = rows[block]
            gate_pre = jnp.dot(entry_rows, gate_mat[...], preferred_element_type=f32)
            up_pre = jnp.dot(entry_rows, up_mat[...], preferred_element_type=f32)
            pulled = lax.dot_general(
                row_cots[block],
                down_mat[...],
                (((1,), (1,)), ((), ())),
                preferred_element_type=f32,
            )
            logistic = jax.nn.sigmoid(gate_pre)
            activated = gate_pre * logistic
            hidden[block] = (activated * up_pre * weight).astype(bf16)
            dhidden = pulled * weight
            grad_gate = (
                dhidden * up_pre * logistic * (1.0 + gate_pre * (1.0 - logistic))
            ).astype(bf16)
            grad_up = (dhidden * activated).astype(bf16)
            dgate[block] = grad_gate
            dup[block] = grad_up

            def back(at, carry):
                picked = columns(at, quarter)
                over_width = (((1,), (1,)), ((), ()))
                partial[block, :, picked] = (
                    lax.dot_general(
                        grad_gate, gate_mat[picked, :], over_width, preferred_element_type=f32
                    )
                    + lax.dot_general(
                        grad_up, up_mat[picked, :], over_width, preferred_element_type=f32
                    )
                ).astype(bf16)
                return carry

            lax.fori_loop(0, lanes, back, 0)
            to_core(block, 1).start()
            to_core(block, 0).start()

        each_block(level, lambda *at: chosen_now(*at, compute))

    def middle_level(level, chosen_now):
        def middle(block, side, line):
            to_core(block, 1).wait_recv()
            to_far[block] = (
                partial[block, :, columns(far_peer, quarter)].astype(f32)
                + from_core[block, 1].astype(f32)
            ).astype(bf16)
            to_far_peer(block).start()

        each_block(level, lambda *at: chosen_now(*at, middle))

    def total_level(level):
        def total(block, side, line):
            to_core(block, 0).wait_recv()
            to_far_peer(block).wait_recv()
            value = (
                partial[block, :, columns(lane, quarter)].astype(f32)
                + from_core[block, 0].astype(f32)
                + from_far[block].astype(f32)
            ).astype(bf16)

            @pl.when(block == spot)
            def _():
                returned[spot] = value

            @pl.when(block != spot)
            def _():
                from_far[block] = value
                home(block).start()

        each_block(level, total)

    slots = groups * span
    down_in = (((0,), (0,)), ((), ()))
    grad_copies = [
        pltpu.make_async_copy(grad_b, down_out, local_sem.at[0]),
        pltpu.make_async_copy(grad_a.at[0], gate_out, local_sem.at[1]),
        pltpu.make_async_copy(grad_a.at[1], up_out, local_sem.at[2]),
    ]

    def down_grad():

        def down_step(at, carry):
            picked = columns(at, quarter)
            grad_b[:, picked] = lax.dot_general(
                hidden[...].reshape(slots, hidden.shape[2]),
                row_cots[:, :, picked].reshape(slots, quarter),
                down_in,
                preferred_element_type=f32,
            )
            return carry

        lax.fori_loop(0, lanes, down_step, 0)
        grad_copies[0].start()

    def wide_grad(spread, index):
        def step(at, carry):
            picked = columns(at, quarter)
            grad_a[index, picked, :] = lax.dot_general(
                rows[:, :, picked].reshape(slots, quarter),
                spread[...].reshape(slots, spread.shape[2]),
                down_in,
                preferred_element_type=f32,
            )
            return carry

        lax.fori_loop(0, lanes, step, 0)
        grad_copies[index + 1].start()

    def advance(level, carry):
        @pl.when(level == 1)
        def _():
            def hear_all(offset, carry):
                told(offset).wait_recv()
                return carry

            lax.fori_loop(1, groups, hear_all, 0)

        take_narrow(level, 1)
        take_narrow(level, 0)
        take_wide(level, 1)
        move_early(level, 0)
        share_level(level - 1)
        work_level(level - 1, False)
        take_wide(level, 0)
        move_early(level + 1, 1)
        work_level(level, True)
        receive_level(level, 1)

        receive_level(level, 0)

        @pl.when(level < depth)
        def _():
            total_level(level - 1)

        return carry

    lax.fori_loop(0, depth + 1, advance, 0)
    down_grad()
    total_level(depth - 1)
    wide_grad(dgate, 0)
    wide_grad(dup, 1)
    combined[...] = jnp.zeros_like(combined)

    def combine_level(level, carry):
        def combine(block, side, line):
            @pl.when(block != spot)
            def _():
                home_from(block).wait_recv()

            combined[...] += lax.dot_general(
                chosen(spot, block), returned[block], down_in, preferred_element_type=f32
            )

        each_block(level, combine)
        return carry

    lax.fori_loop(-1, depth, combine_level, 0)

    def gather_part(who):
        return gathered.at[:, columns(who, quarter)]

    def gather_copy(index, who, peer):
        held = gather_part(who)
        return remote(held, held, send_g.at[index], recv_g.at[index], tp=peer)

    gathered[:, columns(lane, quarter)] = combined[...].astype(bf16)
    gather_copy(0, lane, far_peer).start()
    gather_copy(1, lane, core_peer).start()
    product[...] = jnp.zeros_like(product)

    def add_product(who):
        wide = columns(who, quarter)

        def step(at, carry):
            picked = pl.ds(pl.multiple_of(at * tall, tall), tall)
            pulled = gathered[picked, wide].astype(f32) * gain[:, wide]
            product[picked, :] += jnp.sum(
                pulled * resid[picked, wide].astype(f32), axis=1, keepdims=True
            )
            return carry

        lax.fori_loop(0, token_count // tall, step, 0)

    add_product(lane)
    gather_copy(1, lane, core_peer).wait_recv()
    add_product(core_peer)
    gather_copy(0, lane, far_peer).wait_recv()
    gather_copy(2, far_peer, core_peer).start()
    add_product(far_peer)
    gather_copy(2, far_peer, core_peer).wait_recv()
    add_product(lax.rem(core_peer + lanes // 2, lanes))

    def resid_strip(at, carry):
        picked = pl.ds(pl.multiple_of(at * strip, strip), strip)
        scale = inverse[picked, :]
        pulled = gathered[picked, :].astype(f32) * gain[...]
        shift_back = scale * scale * scale * (product[picked, :] * (1.0 / model_width))
        resid_grad[picked, :] = (
            cots[picked, :].astype(f32)
            + scale * pulled
            - resid[picked, :].astype(f32) * shift_back
        ).astype(bf16)
        return carry

    lax.fori_loop(0, token_count // strip, resid_strip, 0, unroll=2)
    gather_copy(0, lane, far_peer).wait_send()
    gather_copy(1, lane, core_peer).wait_send()
    gather_copy(2, far_peer, core_peer).wait_send()

    @pl.when(spot < groups - 1)
    def _():
        shift().wait_send()

    @pl.when(spot > 0)
    def _():
        shift().wait_recv()

    for copy in grad_copies:
        copy.wait()

    def finish_info(offset, carry):
        tell(offset).wait_send()
        origin = lax.rem(spot + offset, groups)
        home_from(origin).wait_send()
        return carry

    lax.fori_loop(1, groups, finish_info, 0)
    for k in (0, 1):
        for side in (0, 1):

            @pl.when(onward(side))
            def _():
                by_kind(
                    z,
                    lambda: hop_wide(k, z, side, True).wait_send(),
                    lambda: hop(k, z, side, True).wait_send(),
                )

        over_own(k).wait_send()
        half_copy(k, mate).wait_send()

    def finish_level(level, carry):
        def finish(block, side, line):
            to_core(block, 0).wait_send()
            to_core(block, 1).wait_send()
            to_far_peer(block).wait_send()

            @pl.when(level > 0)
            def _():
                at = source(side, level)

                def done(hold, cross):
                    @pl.when(line == 0)
                    def _():
                        for k in (0, 1):
                            cross(k, at).wait_send()

                            @pl.when(onward(side))
                            def _():
                                hold(k, at, side, False).wait_send()

                def wide():
                    for k in (0, 1):
                        half_copy(k, block).wait_send()
                    done(hop_wide, over_wide)

                def narrow():
                    for k in (0, 1):
                        far_copy(k, block).wait_send()
                        core_copy(k, block).wait_send()
                        pass_copy(k, block).wait_send()
                    done(hop, over)

                by_kind(at, wide, narrow)

        each_block(level, finish)
        return carry

    lax.fori_loop(-1, depth, finish_level, 0)


def experts(
    resid,
    cots,
    gain,
    gate_c,
    values_u,
    routes,
    route_weights,
    gate_mat,
    up_mat,
    down_mat,
    groups,
    lanes,
    span,
):
    token_count, model_width = resid.shape
    inner = gate_mat.shape[1]
    quarter = model_width // lanes
    width = 2
    depth = groups // width
    bf16, f32 = jnp.bfloat16, jnp.float32
    dma = pltpu.SemaphoreType.DMA
    inside = pl.BlockSpec(memory_space=pltpu.VMEM)
    anywhere = pl.BlockSpec(memory_space=pl.ANY)
    block = (groups, span, quarter)
    whole = (groups, span, model_width)
    thin = (groups, span, inner)
    edge_shape = (16, gate_c.shape[1])
    vmem = pltpu.VMEM
    return pl.pallas_call(
        functools.partial(expert_kernel, groups, width, lanes),
        out_shape=(
            jax.ShapeDtypeStruct(resid.shape, bf16),
            jax.ShapeDtypeStruct(edge_shape, f32),
            jax.ShapeDtypeStruct(gate_mat.shape, f32),
            jax.ShapeDtypeStruct(up_mat.shape, f32),
            jax.ShapeDtypeStruct(down_mat.shape, f32),
        ),
        in_specs=[inside] * 10,
        out_specs=(inside, inside, anywhere, anywhere, anywhere),
        scratch_shapes=[
            vmem(resid.shape, bf16),
            vmem((token_count, 1), f32),
            vmem((token_count, 1), f32),
            vmem(resid.shape, bf16),
            vmem(edge_shape, f32),
            vmem((groups, 8, token_count), f32),
            vmem((2, depth, token_count, quarter), bf16),
            vmem((2, 2, token_count, model_width // 2), bf16),
            vmem((2, depth, span, quarter), bf16),
            vmem((2, 2, span, model_width // 2), bf16),
            vmem((2, span, model_width // 2), bf16),
            vmem(whole, bf16),
            vmem(whole, bf16),
            vmem(thin, bf16),
            vmem(thin, bf16),
            vmem(thin, bf16),
            vmem(whole, bf16),
            vmem((groups, 2, span, quarter), bf16),
            vmem(block, bf16),
            vmem(block, bf16),
            vmem(block, bf16),
            vmem((token_count, quarter), f32),
            vmem((2,) + gate_mat.shape, f32),
            vmem(down_mat.shape, f32),
            dma((3,)),
            dma((groups,)),
            dma((groups,)),
            dma((2, 2, depth)),
            dma((2, depth)),
            dma((2, depth)),
            dma((2, depth)),
            dma((2,)),
            dma((2,)),
        ]
        + [dma((2, groups))] * 6
        + [dma((groups, 2))] * 2
        + [dma((groups,))] * 4
        + [dma((3,))] * 2
        + [dma((1,))] * 2,
        compiler_params=pltpu.CompilerParams(
            collective_id=1, has_side_effects=True, vmem_limit_bytes=67043328
        ),
        cost_estimate=pl.CostEstimate(
            flops=16 * groups * span * model_width * inner,
            bytes_accessed=150 * 2**20,
            transcendentals=0,
        ),
        name="experts",
    )(
        resid,
        cots,
        gain,
        gate_c,
        values_u,
        routes,
        route_weights,
        gate_mat,
        up_mat,
        down_mat,
    )


def tail_kernel(
    groups,
    width,
    lanes,
    pieces,
    resid_grad,
    earlier,
    out_mat,
    gate_b,
    gate_c,
    values_u,
    taps,
    total,
    grad_b,
    grad_c,
    grad_u,
    partial,
    mixed,
    conv,
    merged,
    pulled,
    edge,
    edge_got,
    from_mate,
    sums,
    arrived,
    send_y,
    recv_y,
    send_z,
    recv_z,
    send_e,
    recv_e,
):
    f32 = jnp.float32
    bf16 = jnp.bfloat16
    spot, lane = lax.axis_index("sp"), lax.axis_index("tp")
    depth = groups // width
    z, y = lax.div(spot, width), lax.rem(spot, width)
    mate = spot + 1 - 2 * y
    core_peer = lane + 1 - 2 * lax.rem(lane, 2)
    far_peer = lax.rem(lane + lanes // 2, lanes)
    token_count, model_width = resid_grad.shape
    piece = model_width // pieces
    per = depth // pieces
    lead = earlier.shape[0]

    def goal_of(step):
        return lax.rem(z + step + 1, depth)

    def over(at):
        return remote(
            partial.at[at * width + 1 - y],
            from_mate.at[at],
            send_y.at[at],
            recv_y.at[at],
            sp=mate,
        )

    def along(at):
        return remote(
            sums.at[at], arrived.at[z], send_z.at[at], recv_z.at[z], sp=at * width + y
        )

    def along_from(at):
        return remote(
            sums.at[at], arrived.at[at], send_z.at[at], recv_z.at[at], sp=at * width + y
        )

    def shift():
        goal = lax.rem(spot + groups - 1, groups)
        return remote(edge, edge_got, send_e.at[0], recv_e.at[0], sp=goal)

    all_here = greet(groups, spot, core_peer, far_peer)
    mixed[0:lead, :] = earlier[...]
    mixed[lead:, :] = gate_c[...].astype(f32) * values_u[...].astype(f32)
    conv[...] = (
        taps[0:1, :] * mixed[lead - 2 : lead - 2 + token_count, :]
        + taps[1:2, :] * mixed[lead - 1 : lead - 1 + token_count, :]
        + taps[2:3, :] * mixed[lead : lead + token_count, :]
    )
    merged[...] = (gate_b[...].astype(f32) * conv[...]).astype(bf16)

    def make(step):
        at = lax.rem(lax.div(z, per) + step + 1, pieces)
        made = lax.dot_general(
            resid_grad[:, pl.ds(pl.multiple_of(at * piece, piece), piece)],
            merged[...],
            (((0,), (0,)), ((), ())),
            preferred_element_type=f32,
        ).astype(bf16)
        count = per * width
        partial[pl.ds(at * count, count)] = made.reshape((count,) + partial.shape[1:])
        return at

    first = make(0)
    all_here()

    def launch(at):
        def step(k, carry):
            over(at * per + k).start()
            return carry

        lax.fori_loop(0, per, step, 0)

    launch(first)

    def make_next(step, carry):
        launch(make(step))
        return carry

    lax.fori_loop(1, pieces, make_next, 0)
    dmerged = jnp.dot(resid_grad[...], out_mat[...], preferred_element_type=f32)
    pulled[0:token_count, :] = dmerged * gate_b[...].astype(f32)
    edge[...] = pulled[0 : edge.shape[0], :]

    @pl.when(spot > 0)
    def _():
        shift().start()

    @pl.when(spot == groups - 1)
    def _():
        edge_got[...] = jnp.zeros_like(edge_got)

    grad_b[...] = (dmerged * conv[...]).astype(bf16)

    def pair(step, carry):
        at = goal_of(step)
        over(at).wait_recv()
        both = partial[at * width + y].astype(f32) + from_mate[at].astype(f32)

        @pl.when(at == z)
        def _():
            total[...] = both

        @pl.when(at != z)
        def _():
            sums[at] = both.astype(sums.dtype)
            along(at).start()

        return carry

    lax.fori_loop(0, depth, pair, 0)

    @pl.when(spot < groups - 1)
    def _():
        shift().wait_recv()

    pulled[token_count:, :] = edge_got[...]
    dmixed = (
        taps[2:3, :] * pulled[0:token_count, :]
        + taps[1:2, :] * pulled[1 : token_count + 1, :]
        + taps[0:1, :] * pulled[2 : token_count + 2, :]
    )
    grad_c[...] = (dmixed * values_u[...].astype(f32)).astype(bf16)
    grad_u[...] = (dmixed * gate_c[...].astype(f32)).astype(bf16)

    def add(step, carry):
        at = lax.rem(z + depth - 1 - step, depth)
        along_from(at).wait_recv()
        total[...] += arrived[at].astype(f32)
        return carry

    lax.fori_loop(0, depth - 1, add, 0)

    def finish(step, carry):
        at = goal_of(step)
        over(at).wait_send()

        @pl.when(at != z)
        def _():
            along(at).wait_send()

        return carry

    lax.fori_loop(0, depth, finish, 0)

    @pl.when(spot > 0)
    def _():
        shift().wait_send()


def tail(resid_grad, earlier, out_mat, gate_b, gate_c, values_u, taps, groups, lanes):
    width = 2
    depth = groups // width
    pieces = lanes if depth % lanes == 0 else 1
    token_count, model_width = resid_grad.shape
    channels = out_mat.shape[1]
    bf16, f32 = jnp.bfloat16, jnp.float32
    dma = pltpu.SemaphoreType.DMA
    vmem = pltpu.VMEM
    inside = pl.BlockSpec(memory_space=vmem)
    block = (model_width // groups, channels)
    flat = (token_count, channels)
    edge_shape = (8, channels)
    held = vmem((depth,) + block, bf16)
    return pl.pallas_call(
        functools.partial(tail_kernel, groups, width, lanes, pieces),
        out_shape=(jax.ShapeDtypeStruct(block, f32),)
        + (jax.ShapeDtypeStruct(flat, bf16),) * 3,
        in_specs=[inside] * 7,
        out_specs=(inside,) * 4,
        scratch_shapes=[
            vmem((groups,) + block, bf16),
            vmem((token_count + earlier.shape[0], channels), f32),
            vmem(flat, f32),
            vmem(flat, bf16),
            vmem((token_count + 8, channels), f32),
            vmem(edge_shape, f32),
            vmem(edge_shape, f32),
            held,
            held,
            held,
        ]
        + [dma((depth,))] * 4
        + [dma((1,))] * 2,
        compiler_params=pltpu.CompilerParams(
            collective_id=4, has_side_effects=True, vmem_limit_bytes=67043328
        ),
        name="tail",
    )(resid_grad, earlier, out_mat, gate_b, gate_c, values_u, taps)


def hand_kernel(count, parts, *refs):
    given, out, held = refs[:count], refs[count : 2 * count], refs[2 * count : 3 * count]
    come, go = refs[3 * count :]

    def piece(ref, at):
        step = ref.shape[0] // parts
        return ref.at[at * step : (at + 1) * step]

    def inward(k, at):
        return pltpu.make_async_copy(piece(given[k], at), piece(held[k], at), come.at[k, at])

    def outward(k, at):
        return pltpu.make_async_copy(piece(held[k], at), piece(out[k], at), go.at[k, at])

    every = [(k, at) for k in range(count) for at in range(parts)]
    for k, at in every:
        inward(k, at).start()
    for k, at in every:
        inward(k, at).wait()
        outward(k, at).start()
    for k, at in every:
        outward(k, at).wait()


def hand_over(*arrays):
    parts = 4
    count = len(arrays)
    anywhere = pl.BlockSpec(memory_space=pl.ANY)
    dma = pltpu.SemaphoreType.DMA((count, parts))
    return pl.pallas_call(
        functools.partial(hand_kernel, count, parts),
        out_shape=tuple(jax.ShapeDtypeStruct(a.shape, a.dtype) for a in arrays),
        in_specs=[anywhere] * count,
        out_specs=(anywhere,) * count,
        scratch_shapes=[pltpu.VMEM(a.shape, a.dtype) for a in arrays] + [dma, dma],
        compiler_params=pltpu.CompilerParams(vmem_limit_bytes=67043328),
        name="hand_over",
    )(*arrays)


def on_device(
    resid_in,
    cotangent,
    norm_gain,
    routes,
    route_weights,
    gate_weight,
    up_weight,
    down_weight,
    out_weight,
    gate_b,
    gate_c,
    values_u,
    taps,
):
    groups = lax.axis_size("sp")
    lanes = lax.axis_size("tp")
    expert_total = gate_weight.shape[0] * groups
    capacity = 4 * resid_in.shape[0] // expert_total
    grad_resid, earlier, grad_gate, grad_up, grad_down = experts(
        resid_in,
        cotangent,
        norm_gain[None, :],
        gate_c,
        values_u,
        routes.T,
        route_weights.T,
        gate_weight[0],
        up_weight[0],
        down_weight[0],
        groups,
        lanes,
        gate_weight.shape[0] * capacity,
    )
    given = tail(
        grad_resid, earlier, out_weight, gate_b, gate_c, values_u, taps, groups, lanes
    )
    results = hand_over(grad_gate, grad_up, grad_down, grad_resid, *given)
    return tuple(array[None] for array in results[:3]) + tuple(results[3:])


def solution(mesh):
    placed = (
        P("sp", None),
        P("sp", None),
        P(),
        P("sp", None),
        P("sp", None),
        P("sp", None, "tp"),
        P("sp", None, "tp"),
        P("sp", "tp", None),
        P(None, "tp"),
        P("sp", "tp"),
        P("sp", "tp"),
        P("sp", "tp"),
        P(None, "tp"),
    )
    return jax.shard_map(
        on_device,
        mesh=mesh,
        in_specs=placed,
        out_specs=(
            P("sp", None, "tp"),
            P("sp", None, "tp"),
            P("sp", "tp", None),
            P("sp", None),
            P("sp", "tp"),
            P("sp", "tp"),
            P("sp", "tp"),
            P("sp", "tp"),
        ),
        check_vma=False,
    )
```
